128 devices in a mesh: ep: 128 (over z, y, x, core).
Axes of the slice: x: 4, y: 4, z: 4, core: 2. Of those that a mesh axis runs over, the one named last changes fastest.
Arguments:
- tokens: bfloat16 [2048, 1024], P('ep'), may hold values from -6 to 6
- lengths: int32 [2048], P('ep'), may hold values from 1 to 8191
- cache_keys: bfloat16 [2048, 128, 512], P('ep'), may hold values from -6 to 6
- cache_values: bfloat16 [2048, 128, 1024], P('ep'), may hold values from -6 to 6
- retention_state: float32 [2048, 4, 128, 256], P('ep'), may hold values from -24 to 24
- mix_gain: float32 [1024], replicated, may hold values from 0.1 to 1.9
- query_weight: bfloat16 [1024, 512], replicated, may hold values from -0.1875 to 0.1875
- key_weight: bfloat16 [1024, 512], replicated, may hold values from -0.1875 to 0.1875
- value_weight: bfloat16 [1024, 1024], replicated, may hold values from -0.1875 to 0.1875
- out_weight: bfloat16 [1024, 1024], replicated, may hold values from -0.1875 to 0.1875
- ffn_gain: float32 [1024], replicated, may hold values from 0.1 to 1.9
- routes: int32 [2048, 6], P('ep'), may hold values from 0 to 127, all different within a row; in each aligned block of 16 rows (0 to 15, 16 to 31, ...) at most 2 rows name the same one
- route_scores: float32 [2048, 6], P('ep'), may hold values from 0.05 to 1
- expert_gate: bfloat16 [128, 1024, 256], P('ep'), may hold values from -0.1875 to 0.1875
- expert_up: bfloat16 [128, 1024, 256], P('ep'), may hold values from -0.1875 to 0.1875
- expert_down: bfloat16 [128, 256, 1024], P('ep'), may hold values from -0.375 to 0.375
- shared_gate: bfloat16 [1024, 256], replicated, may hold values from -0.1875 to 0.1875
- shared_up: bfloat16 [1024, 256], replicated, may hold values from -0.1875 to 0.1875
- shared_down: bfloat16 [256, 1024], replicated, may hold values from -0.375 to 0.375
- dense_gate: bfloat16 [4096, 1024], P('ep'), may hold values from -0.1875 to 0.1875
- dense_up: bfloat16 [4096, 1024], P('ep'), may hold values from -0.1875 to 0.1875
- dense_down: bfloat16 [4096, 1024], P('ep'), may hold values from -0.09375 to 0.09375
- dense_mix: float32 [1024], replicated, may hold values from -3 to 3
Outputs:
- layer_out: bfloat16 [2048, 1024], P('ep')
- new_keys: bfloat16 [2048, 512], P('ep')
- new_values: bfloat16 [2048, 1024], P('ep')
The draws below stay inside these ranges and needn't reach their ends.
Inputs may be any that keep to these rules, and one draw needn't show every extreme that they name: `routes`: each row names 6 different experts; among the rows of one device no expert is named more than 2 times.
All inputs are finite; a program needn't handle non-finite values.
Results may differ from the reference program's by a relative error of at most 0.012.
Values may be sent and summed in bfloat16 or wider, within the bound.
A program may use at most 128 MiB of HBM per device.

```python
import math
import jax
import jax.numpy as jnp
import numpy as np
from jax import lax

D = 1024
HEADS = 4
DK = 128
DV = 256
BLOCK = 128
SEQ_DEV = 16
SEQS = 2048
EXPERTS = 128
TOP_K = 6
CAP = 2
EH = 256
SH = 256
DENSE_FF = 4096
N_EP = 128


def plant(values, stream_key, smallest, top_value):
    dims = values.shape
    spot = [jax.random.randint(jax.random.fold_in(stream_key, axis), (), 0, dims[axis]) for axis in range(len(dims))]
    values = values.at[tuple(spot)].set(smallest)
    longest = dims.index(max(dims))
    spot[longest] = (spot[longest] + 1) % dims[longest]
    return values.at[tuple(spot)].set(top_value)


def shard_levels(rng, dims, shards, low, high):
    factor_of = 1.0
    for axis_at, shards_of in shards:
        heights = jax.random.uniform(jax.random.fold_in(jax.random.fold_in(rng, 6), axis_at), (shards_of,), jnp.float32, low / len(shards), high / len(shards))
        factor_of = factor_of * jnp.repeat(jnp.exp(heights), dims[axis_at] // shards_of).reshape((-1,) + (1,) * (len(dims) - 1 - axis_at))
    return factor_of


def routed_block(key, own, number, rows, count, top, reach, slope):
    sequence = jax.random.permutation(key, count)
    crowded, common = portions_of(count, rows * top, reach, slope, True), portions_of(count, rows * top, reach, slope, False)
    places = jnp.arange(count)

    def named(tallies, offset_by):
        used = int((tallies > 0).sum())
        fixed = max(1, used // 4)
        passed = fixed + (places - fixed + offset_by * (used - fixed)) % max(1, count - fixed)
        return jnp.zeros((count,), jnp.int32).at[sequence[jnp.where(places < fixed, places, passed)]].set(jnp.asarray(tallies, jnp.int32))

    tallies = jnp.where(number % 4 == 0, named(crowded, number // 4), named(common, number - number // 4 - 1))
    mixed = jax.random.permutation(jax.random.fold_in(own, 3), count)
    donor, receiver = mixed[0:count // 2 * 2:2], mixed[1:count // 2 * 2:2]
    room = jnp.minimum(tallies[donor] - 1, reach - tallies[receiver]) // 2
    room = jnp.where((donor == sequence[0]) | (receiver == sequence[0]) | (tallies[receiver] == 0), 0, jnp.maximum(room, 0))
    passed = jax.random.randint(jax.random.fold_in(own, 4), (count // 2,), 0, 1 << 20) % (room + 1)
    tallies = tallies.at[donor].add(-passed).at[receiver].add(passed)
    members = jnp.searchsorted(jnp.cumsum(tallies), jnp.arange(rows * top), side="right").astype(jnp.int32)
    grid = members.reshape(top, rows).T
    grid = grid[jax.random.permutation(jax.random.fold_in(own, 1), rows)]
    offset_by = jax.random.randint(jax.random.fold_in(own, 2), (rows, 1), 0, top)
    return jnp.take_along_axis(grid, (jnp.arange(top)[None, :] + offset_by) % top, axis=1)


def portions_of(amount, total, limit, slope, full):
    portions = [(1 << 20) // math.isqrt(grade ** slope) + 1 for grade in range(1, amount + 1)]
    largest = limit if full else min(limit, max(-(-total // amount), total * portions[0] // sum(portions)))
    least = 1 if total - largest >= amount - 1 else 0
    counts, surplus = [largest] + [least] * (amount - 1), total - largest - least * (amount - 1)
    while surplus > 0:
        free = [i for i in range(1, amount) if counts[i] < largest] or [i for i in range(1, amount) if counts[i] < limit]
        pool, budget = sum([portions[i] for i in free]), surplus
        for i in free:
            addition = min(limit - counts[i], max(1, budget * portions[i] // pool), surplus)
            counts[i] = counts[i] + addition
            surplus = surplus - addition
    return np.array(counts)


def gaussian(own_key, dims, deviation, reach, shards=(), held_as=jnp.bfloat16):
    result = deviation * jax.random.normal(own_key, dims, jnp.float32)
    if shards:
        result = result * shard_levels(own_key, dims, shards, -0.22, 0.18)
    return jnp.clip(result, -reach, reach).astype(held_as)


def setup_inputs(seed: int = 0) -> dict:
    key_of = jax.random.split(jax.random.key(seed), 24)
    tokens = gaussian(key_of[0], (SEQS, D), 1.0, 6.0, ((0, 128),))
    lengths = plant(jax.random.randint(key_of[1], (SEQS,), 1, 8192), jax.random.fold_in(key_of[1], 1), 1, 8191).astype(jnp.int32)
    cache_keys = gaussian(key_of[2], (SEQS, BLOCK, HEADS * DK), 1.0, 6.0, ((0, 128),))
    cache_values = gaussian(key_of[3], (SEQS, BLOCK, HEADS * DV), 1.0, 6.0, ((0, 128),))
    retention_state = gaussian(key_of[4], (SEQS, HEADS, DK, DV), 4.0, 24.0, ((0, 128),), jnp.float32)
    mix_gain = jnp.clip(1.0 + 0.18 * jax.random.normal(key_of[5], (D,), jnp.float32), 0.1, 1.9)
    query_weight = gaussian(key_of[6], (D, HEADS * DK), D ** -0.5, 0.1875)
    key_weight = gaussian(key_of[7], (D, HEADS * DK), D ** -0.5, 0.1875)
    value_weight = gaussian(key_of[8], (D, HEADS * DV), D ** -0.5, 0.1875)
    out_weight = gaussian(key_of[9], (HEADS * DV, D), (HEADS * DV) ** -0.5, 0.1875)
    ffn_gain = jnp.clip(1.0 + 0.18 * jax.random.normal(key_of[10], (D,), jnp.float32), 0.1, 1.9)
    routes_keys = jax.random.split(jax.random.fold_in(key_of[11], 1), SEQS // SEQ_DEV)
    routes_turns = jax.random.permutation(jax.random.fold_in(key_of[11], 3), SEQS // SEQ_DEV)
    routes = jax.vmap(lambda own, number: routed_block(jax.random.fold_in(key_of[11], 2), own, number, SEQ_DEV, EXPERTS, TOP_K, CAP, 1))(routes_keys, routes_turns).reshape((SEQS, TOP_K))
    route_scores = jnp.clip(0.05 + 0.95 * jax.random.uniform(key_of[12], (SEQS, TOP_K), jnp.float32) ** shard_levels(key_of[12], (SEQS, TOP_K), ((0, 128),), -0.2, 0.2), 0.05, 1.0)
    expert_gate = gaussian(key_of[13], (EXPERTS, D, EH), D ** -0.5, 0.1875, ((0, 128),))
    expert_up = gaussian(key_of[14], (EXPERTS, D, EH), D ** -0.5, 0.1875, ((0, 128),))
    expert_down = gaussian(key_of[15], (EXPERTS, EH, D), EH ** -0.5, 0.375, ((0, 128),))
    shared_gate = gaussian(key_of[16], (D, SH), D ** -0.5, 0.1875)
    shared_up = gaussian(key_of[17], (D, SH), D ** -0.5, 0.1875)
    shared_down = gaussian(key_of[18], (SH, D), SH ** -0.5, 0.375)
    dense_gate = gaussian(key_of[19], (DENSE_FF, D), D ** -0.5, 0.1875, ((0, 128),))
    dense_up = gaussian(key_of[20], (DENSE_FF, D), D ** -0.5, 0.1875, ((0, 128),))
    dense_down = gaussian(key_of[21], (DENSE_FF, D), DENSE_FF ** -0.5, 0.09375, ((0, 128),))
    dense_mix = jnp.clip(jax.random.uniform(key_of[22], (D,), jnp.float32, -3.0, 3.0), -3.0, 3.0)
    return {"tokens": tokens, "lengths": lengths, "cache_keys": cache_keys, "cache_values": cache_values, "retention_state": retention_state, "mix_gain": mix_gain, "query_weight": query_weight, "key_weight": key_weight, "value_weight": value_weight, "out_weight": out_weight, "ffn_gain": ffn_gain, "routes": routes, "route_scores": route_scores, "expert_gate": expert_gate, "expert_up": expert_up, "expert_down": expert_down, "shared_gate": shared_gate, "shared_up": shared_up, "shared_down": shared_down, "dense_gate": dense_gate, "dense_up": dense_up, "dense_down": dense_down, "dense_mix": dense_mix}


eps = 1e-06
route_scale = 2.5
rope_base = 10000.0

def normed(values):
    return values * lax.rsqrt(lax.optimization_barrier(jnp.mean(values * values, axis=-1, keepdims=True)) + eps)

def log_decay(head_count):
    return jnp.log1p(-jnp.exp2(-5.0 - jnp.arange(head_count, dtype=jnp.float32)))

def rotate(values, positions):
    half_size = values.shape[-1] // 2
    inverse = rope_base ** (-jnp.arange(half_size, dtype=jnp.float32) / half_size)
    angles = positions.astype(jnp.float32)[:, None, None] * inverse[None, None, :]
    cosine = jnp.cos(angles)
    sine_part = jnp.sin(angles)
    first_half = values[..., :half_size]
    second = values[..., half_size:]
    return jnp.concatenate([first_half * cosine - second * sine_part, first_half * sine_part + second * cosine], axis=-1)

def swiglu(inputs, w_gate, w_up, w_down):
    gate_part = jnp.dot(inputs, w_gate, preferred_element_type=jnp.float32)
    up_part = jnp.dot(inputs, w_up, preferred_element_type=jnp.float32)
    hidden = (jax.nn.silu(gate_part) * up_part).astype(jnp.bfloat16)
    return jnp.dot(hidden, w_down, preferred_element_type=jnp.float32)

def retain(tokens, lengths, mix_gain, w_query, w_key, w_value, w_out, cache_keys, cache_values, carry_state):
    seq_count, head_count, key_size, value_size = carry_state.shape
    block_size = cache_keys.shape[1]
    widened = tokens.astype(jnp.float32)
    normal_in = (normed(widened) * mix_gain).astype(jnp.bfloat16)
    raw_query = jnp.dot(normal_in, w_query, preferred_element_type=jnp.float32).reshape(seq_count, head_count, key_size)
    raw_key = jnp.dot(normal_in, w_key, preferred_element_type=jnp.float32).reshape(seq_count, head_count, key_size)
    raw_value = jnp.dot(normal_in, w_value, preferred_element_type=jnp.float32).reshape(seq_count, head_count, value_size)
    queries = (rotate(raw_query, lengths) * key_size ** (-0.5)).astype(jnp.bfloat16)
    new_keys = rotate(raw_key, lengths).astype(jnp.bfloat16)
    new_values = raw_value.astype(jnp.bfloat16)
    filled = lengths % block_size
    decay_rate = log_decay(head_count)
    places = jnp.arange(block_size, dtype=jnp.int32)
    stored_keys = cache_keys.reshape(seq_count, block_size, head_count, key_size)
    stored_values = cache_values.reshape(seq_count, block_size, head_count, value_size)
    scores = jnp.einsum('shd,sjhd->shj', queries.astype(jnp.float32), stored_keys.astype(jnp.float32))
    distance = jnp.maximum(filled[:, None] - places[None, :], 0).astype(jnp.float32)
    live_mask = places[None, :] < filled[:, None]
    weighted = jnp.where(live_mask[:, None, :], scores * jnp.exp(distance[:, None, :] * decay_rate[None, :, None]), 0.0).astype(jnp.bfloat16)
    own_weight = lax.optimization_barrier(jnp.sum(queries.astype(jnp.float32) * new_keys.astype(jnp.float32), axis=-1)).astype(jnp.bfloat16)
    inside = jnp.einsum('shj,sjhe->she', weighted.astype(jnp.float32), stored_values.astype(jnp.float32))
    inside = inside + own_weight.astype(jnp.float32)[:, :, None] * new_values.astype(jnp.float32)
    carried = jnp.einsum('shd,shde->she', queries.astype(jnp.float32), carry_state, precision=lax.Precision.HIGHEST)
    carried = carried * jnp.exp((filled.astype(jnp.float32)[:, None] + 1.0) * decay_rate[None, :])[:, :, None]
    headed = normed(inside + carried).astype(jnp.bfloat16).reshape(seq_count, head_count * value_size)
    mixer_out = jnp.dot(headed, w_out, preferred_element_type=jnp.float32)
    residual = widened + normed(mixer_out)
    return (residual, new_keys.reshape(seq_count, head_count * key_size), new_values.reshape(seq_count, head_count * value_size))

def reference(tokens, lengths, cache_keys, cache_values, retention_state, mix_gain, query_weight, key_weight, value_weight, out_weight, ffn_gain, routes, route_scores, expert_gate, expert_up, expert_down, shared_gate, shared_up, shared_down, dense_gate, dense_up, dense_down, dense_mix):
    residual, new_keys, new_values = retain(tokens, lengths, mix_gain, query_weight, key_weight, value_weight, out_weight, cache_keys, cache_values, retention_state)
    normal_ffn = (normed(residual) * ffn_gain).astype(jnp.bfloat16)
    shared_out = swiglu(normal_ffn, shared_gate, shared_up, shared_down)
    dense_gate_part = jnp.dot(normal_ffn, dense_gate.T, preferred_element_type=jnp.float32)
    dense_up_part = jnp.dot(normal_ffn, dense_up.T, preferred_element_type=jnp.float32)
    dense_hidden = (jax.nn.silu(dense_gate_part) * dense_up_part).astype(jnp.bfloat16)
    dense_out = jnp.dot(dense_hidden, dense_down, preferred_element_type=jnp.float32)
    route_weight = route_scores / lax.optimization_barrier(jnp.sum(route_scores, axis=-1, keepdims=True)) * route_scale
    flat_routes = routes.reshape(-1)
    flat_weight = route_weight.reshape(-1)
    most_rows = N_EP * CAP
    slot_rank = jnp.arange(most_rows, dtype=jnp.int32)

    def one_expert(running, expert_id):
        hits = flat_routes == expert_id
        hit_count = jnp.sum(hits.astype(jnp.int32))
        picked = jnp.nonzero(hits, size=most_rows, fill_value=0)[0].astype(jnp.int32)
        is_valid = slot_rank < hit_count
        row_ids = picked // TOP_K
        outputs = swiglu(normal_ffn[row_ids], expert_gate[expert_id], expert_up[expert_id], expert_down[expert_id]).astype(jnp.bfloat16)
        added = jnp.where(is_valid[:, None], outputs.astype(jnp.float32) * flat_weight[picked][:, None], 0.0)
        return (running.at[row_ids].add(added), None)
    routed, _ = lax.scan(one_expert, jnp.zeros(residual.shape, jnp.float32), jnp.arange(EXPERTS, dtype=jnp.int32))
    combined = shared_out + routed + jax.nn.sigmoid(dense_mix) * dense_out
    layer_out = (residual + normed(combined)).astype(jnp.bfloat16)
    return (layer_out, new_keys, new_values)
```

```python
import jax
import jax.numpy as jnp
from jax import lax
from jax.experimental import pallas as pl
from jax.experimental.pallas import tpu as pltpu
from jax.sharding import PartitionSpec as P

eps = 1e-06
route_scale = 2.5
rope_base = 10000.0
MESH = pl.DeviceIdType.MESH
BF = jnp.bfloat16
F32 = jnp.float32


def normed(values):
    return values * lax.rsqrt(jnp.mean(values * values, axis=-1, keepdims=True) + eps)


def log_decay(head_count):
    return jnp.log1p(-jnp.exp2(-5.0 - jnp.arange(head_count, dtype=jnp.float32)))


def rotate(values, positions):
    half_size = values.shape[-1] // 2
    inverse = rope_base ** (-jnp.arange(half_size, dtype=jnp.float32) / half_size)
    angles = positions.astype(jnp.float32)[:, None, None] * inverse[None, None, :]
    cosine = jnp.cos(angles)
    sine_part = jnp.sin(angles)
    first_half = values[..., :half_size]
    second = values[..., half_size:]
    return jnp.concatenate(
        [first_half * cosine - second * sine_part, first_half * sine_part + second * cosine],
        axis=-1,
    )


def retain(
    tokens, lengths, mix_gain, w_query, w_key, w_value, w_out, cache_keys, cache_values, carry_state
):
    seq_count, head_count, key_size, value_size = carry_state.shape
    block_size = cache_keys.shape[1]
    widened = tokens.astype(jnp.float32)
    normal_in = (normed(widened) * mix_gain).astype(jnp.bfloat16)
    raw_query = jnp.dot(normal_in, w_query, preferred_element_type=jnp.float32).reshape(
        seq_count, head_count, key_size
    )
    raw_key = jnp.dot(normal_in, w_key, preferred_element_type=jnp.float32).reshape(
        seq_count, head_count, key_size
    )
    raw_value = jnp.dot(normal_in, w_value, preferred_element_type=jnp.float32).reshape(
        seq_count, head_count, value_size
    )
    queries = (rotate(raw_query, lengths) * key_size ** (-0.5)).astype(jnp.bfloat16)
    new_keys = rotate(raw_key, lengths).astype(jnp.bfloat16)
    new_values = raw_value.astype(jnp.bfloat16)
    filled = lengths % block_size
    decay_rate = log_decay(head_count)
    places = jnp.arange(block_size, dtype=jnp.int32)
    stored_keys = cache_keys.reshape(seq_count, block_size, head_count, key_size)
    stored_values = cache_values.reshape(seq_count, block_size, head_count, value_size)
    scores = jnp.einsum("shd,sjhd->shj", queries, stored_keys, preferred_element_type=jnp.float32)
    distance = jnp.maximum(filled[:, None] - places[None, :], 0).astype(jnp.float32)
    live_mask = places[None, :] < filled[:, None]
    weighted = jnp.where(
        live_mask[:, None, :],
        scores * jnp.exp(distance[:, None, :] * decay_rate[None, :, None]),
        0.0,
    ).astype(jnp.bfloat16)
    own_weight = jnp.sum(
        queries.astype(jnp.float32) * new_keys.astype(jnp.float32), axis=-1
    ).astype(jnp.bfloat16)
    inside = jnp.einsum(
        "shj,sjhe->she", weighted, stored_values, preferred_element_type=jnp.float32
    )
    inside = inside + own_weight.astype(jnp.float32)[:, :, None] * new_values.astype(jnp.float32)
    carried = jnp.einsum("shd,shde->she", queries.astype(jnp.float32), carry_state)
    carried = (
        carried
        * jnp.exp((filled.astype(jnp.float32)[:, None] + 1.0) * decay_rate[None, :])[:, :, None]
    )
    headed = (
        normed(inside + carried).astype(jnp.bfloat16).reshape(seq_count, head_count * value_size)
    )
    mixer_out = jnp.dot(headed, w_out, preferred_element_type=jnp.float32)
    residual = widened + normed(mixer_out)
    return (
        residual,
        new_keys.reshape(seq_count, head_count * key_size),
        new_values.reshape(seq_count, head_count * value_size),
    )


def dot(a, b):
    return jnp.dot(a, b, preferred_element_type=F32)


def dot_t(a, b):
    return lax.dot_general(a, b, (((1,), (1,)), ((), ())), preferred_element_type=F32)


def silu(v):
    return v / (1.0 + jnp.exp(-v))


def iota(shape, dim):
    return lax.broadcasted_iota(jnp.int32, shape, dim)


def ffn_kernel(
    x_ref, res_ref, routes_ref, scores_ref, mix_ref,
    eg_hbm, eu_hbm, ed_hbm, sg_hbm, su_hbm, sd_hbm, dg_hbm, du_hbm, dd_hbm,
    out_ref,
    xg, wg, dw, sbuf, rbuf, ybuf, bbuf, pbuf, qbuf,
    eg, eu, ed, sg, su, sd,
    loc, lw, w_s, w_r, d_s, d_r, x_s, x_r, a_s, a_r, b_s, b_r, p_s, p_r,
):
    me = lax.axis_index("ep")
    q = lax.rem(me, 8)
    p = lax.div(me, 8)
    z = lax.div(p, 4)
    y = lax.rem(p, 4)
    base = me - q

    def mate(k):
        return lax.rem(q + k, 8)

    def plane(dz, dy):
        return lax.rem(z + dz, 4), lax.rem(y + dy, 4)

    def device(zz, yy):
        return (zz * 4 + yy) * 8 + q

    def remote(src, dst, s, r, dev):
        return pltpu.make_async_remote_copy(
            src_ref=src, dst_ref=dst, send_sem=s, recv_sem=r, device_id=(dev,), device_id_type=MESH
        )

    barrier = pltpu.get_barrier_semaphore()
    for k in range(1, 8):
        pl.semaphore_signal(barrier, inc=1, device_id=(base + mate(k),), device_id_type=MESH)
    offsets = [(dz, dy) for dz in (0, 1, 3, 2) for dy in (0, 1, 3, 2) if (dz, dy) != (0, 0)]
    for dz, dy in offsets:
        pl.semaphore_signal(barrier, inc=1, device_id=(device(*plane(dz, dy)),), device_id_type=MESH)

    own = []
    for i, hbm in enumerate((dg_hbm, du_hbm, dd_hbm)):
        for h in range(2):
            own.append(
                pltpu.make_async_copy(
                    hbm.at[pl.ds(16 * h, 16)], dw.at[i, z, y, h], loc.at[2 * i + h]
                )
            )
    fetch = []
    for i, (hbm, ref) in enumerate(
        ((sg_hbm, sg), (su_hbm, su), (sd_hbm, sd), (eg_hbm.at[0], eg), (eu_hbm.at[0], eu), (ed_hbm.at[0], ed))
    ):
        fetch.append(pltpu.make_async_copy(hbm, ref, lw.at[i]))
    for c in own + fetch:
        c.start()

    scores = scores_ref[...]
    weight = scores / jnp.sum(scores, axis=-1, keepdims=True) * route_scale
    lanes = iota((16, 128), 1)
    spread = jnp.zeros((16, 128), F32)
    for k in range(6):
        spread = jnp.where(routes_ref[:, k : k + 1] == lanes, weight[:, k : k + 1], spread)
    wg[q] = spread
    xg[q] = x_ref[...]

    pl.semaphore_wait(barrier, 22)

    x_copies, w_copies = [], []
    for k in range(1, 8):
        w_copies.append(remote(wg.at[q], wg.at[q], w_s.at[k], w_r.at[k], base + mate(k)))
        x_copies.append(remote(x_ref, xg.at[q], x_s.at[k], x_r.at[k], base + mate(k)))
    for c in x_copies + w_copies:
        c.start()

    for c in own:
        c.wait()

    def ring(part, step):
        copies = []
        for half in range(2):
            for sign in range(2):
                away = 1 if sign == 0 else 3
                along_y = (half == 0) == (part == 0)
                dev = device(*(plane(0, away) if along_y else plane(away, 0)))
                back = 0 if step == 0 else (4 - away)
                zz, yy = plane(0, back) if along_y else plane(back, 0)
                cols = pl.ds(0, 1024) if step == 0 else pl.ds(512 * sign, 512)
                if part == 0:
                    block = dw.at[:, zz, yy, half, :, cols]
                elif along_y:
                    block = dw.at[:, :, yy, half, :, cols]
                else:
                    block = dw.at[:, zz, :, half, :, cols]
                i = part * 8 + step * 4 + half * 2 + sign
                copies.append(remote(block, block, d_s.at[i], d_r.at[i], dev))
        return copies

    rings = [ring(0, 0), ring(0, 1), ring(1, 0), ring(1, 1)]
    for c in rings[0]:
        c.start()

    for c in fetch[:3]:
        c.wait()
    xv = x_ref[...]
    hidden = (silu(dot(xv, sg[...])) * dot(xv, su[...])).astype(BF)
    shared = dot(hidden, sd[...])

    for c in rings[0]:
        c.wait_recv()
    for c in rings[1]:
        c.start()

    for c in w_copies:
        c.wait_recv()
    w_t = wg[...].reshape(128, 128).T
    before = (iota((128, 128), 0) < iota((128, 128), 1)) & (
        iota((128, 128), 0) // 16 == iota((128, 128), 1) // 16
    )
    rank = dot(jnp.where(w_t > 0, 1.0, 0.0).astype(BF), jnp.where(before, 1.0, 0.0).astype(BF))
    mine = iota((16, 8, 128), 1) == q
    w_p = jnp.sum(jnp.where(mine, w_t.reshape(16, 8, 128), 0.0), axis=1)
    r_p = jnp.sum(jnp.where(mine, rank.reshape(16, 8, 128), 0.0), axis=1)
    slot = iota((16, 16, 128), 1)
    tok = iota((16, 16, 128), 2)
    w_b = jnp.broadcast_to(w_p[:, None, :], (16, 16, 128))
    r_b = jnp.broadcast_to(r_p[:, None, :], (16, 16, 128))
    fits = (slot // 2 == tok // 16) & (r_b == (slot % 2).astype(F32))
    picked = jnp.where(fits, w_b, 0.0).reshape(256, 128)
    choose = jnp.where(picked > 0, 1.0, 0.0).astype(BF)
    combine = picked.T
    comb_hi = combine.astype(BF)
    comb_lo = (combine - comb_hi.astype(F32)).astype(BF)

    for c in x_copies:
        c.wait_recv()
    xall = xg[...].reshape(128, 1024)
    sbuf[...] = dot(choose, xall).astype(BF).reshape(4, 4, 16, 1024)
    out_copies = {}
    for dz, dy in offsets:
        zz, yy = plane(dz, dy)
        i = dz * 4 + dy
        out_copies[i] = remote(
            sbuf.at[zz, yy], rbuf.at[z, y], a_s.at[i], a_r.at[i], device(zz, yy)
        )
        out_copies[i].start()
    rbuf[z, y] = sbuf[z, y]

    for c in rings[1]:
        c.wait_recv()
    for c in rings[2]:
        c.start()

    for c in fetch[3:]:
        c.wait()
    back_copies = {}
    for dz in (0, 1, 3, 2):
        for dy in range(4):
            if (dz, dy) != (0, 0):
                out_copies[dz * 4 + dy].wait_recv()
        zz = lax.rem(z + 4 - dz, 4)
        rows = rbuf[zz].reshape(64, 1024)
        hid = (silu(dot(rows, eg[...])) * dot(rows, eu[...])).astype(BF)
        ybuf[zz] = dot(hid, ed[...]).astype(BF).reshape(4, 16, 1024)
        for dy in (0, 1, 3, 2):
            if (dz, dy) != (0, 0):
                yy = lax.rem(y + 4 - dy, 4)
                i = dz * 4 + dy
                back_copies[i] = remote(
                    ybuf.at[zz, yy], bbuf.at[z, y], b_s.at[i], b_r.at[i], device(zz, yy)
                )
                back_copies[i].start()
    bbuf[z, y] = ybuf[z, y]

    for c in rings[2]:
        c.wait_recv()
    for c in rings[3]:
        c.start()
    for c in rings[3]:
        c.wait_recv()

    gate = dot_t(xall, dw[0].reshape(512, 1024))
    up = dot_t(xall, dw[1].reshape(512, 1024))
    dense = dot((silu(gate) * up).astype(BF), dw[2].reshape(512, 1024))
    mix = mix_ref[...]
    partial = dense * (1.0 / (1.0 + jnp.exp(-mix)))

    for i in back_copies:
        back_copies[i].wait_recv()
    back = bbuf[...].reshape(256, 1024)
    partial = partial + dot(comb_hi, back) + dot(comb_lo, back)
    pbuf[...] = partial.astype(BF).reshape(8, 16, 1024)
    p_copies = []
    for k in range(1, 8):
        p_copies.append(
            remote(pbuf.at[mate(k)], qbuf.at[q], p_s.at[k], p_r.at[k], base + mate(k))
        )
    for c in p_copies:
        c.start()
    qbuf[q] = pbuf[q]
    for c in p_copies:
        c.wait_recv()
    total = shared + jnp.sum(qbuf[...].astype(F32), axis=0)
    out_ref[...] = (res_ref[...] + normed(total)).astype(BF)

    for c in w_copies + x_copies + p_copies:
        c.wait_send()
    for r in rings:
        for c in r:
            c.wait_send()
    for group in (out_copies, back_copies):
        for i in group:
            group[i].wait_send()


def exchange(x, residual, routes, scores, mix, eg, eu, ed, sg, su, sd, dg, du, dd):
    vm = pl.BlockSpec(memory_space=pltpu.VMEM)
    hbm = pl.BlockSpec(memory_space=pl.ANY)
    dma = pltpu.SemaphoreType.DMA
    return pl.pallas_call(
        ffn_kernel,
        out_shape=jax.ShapeDtypeStruct((16, 1024), BF),
        in_specs=[vm] * 5 + [hbm] * 9,
        out_specs=vm,
        scratch_shapes=[
            pltpu.VMEM((8, 16, 1024), BF),
            pltpu.VMEM((8, 16, 128), F32),
            pltpu.VMEM((3, 4, 4, 2, 16, 1024), BF),
            pltpu.VMEM((4, 4, 16, 1024), BF),
            pltpu.VMEM((4, 4, 16, 1024), BF),
            pltpu.VMEM((4, 4, 16, 1024), BF),
            pltpu.VMEM((4, 4, 16, 1024), BF),
            pltpu.VMEM((8, 16, 1024), BF),
            pltpu.VMEM((8, 16, 1024), BF),
            pltpu.VMEM((1024, 256), BF),
            pltpu.VMEM((1024, 256), BF),
            pltpu.VMEM((256, 1024), BF),
            pltpu.VMEM((1024, 256), BF),
            pltpu.VMEM((1024, 256), BF),
            pltpu.VMEM((256, 1024), BF),
            dma((6,)), dma((6,)), dma((8,)), dma((8,)), dma((16,)), dma((16,)),
            dma((8,)), dma((8,)), dma((16,)), dma((16,)), dma((16,)), dma((16,)),
            dma((8,)), dma((8,)),
        ],
        compiler_params=pltpu.CompilerParams(collective_id=0, has_side_effects=True),
    )(x, residual, routes, scores, mix, eg, eu, ed, sg, su, sd, dg, du, dd)


def per_device(
    tokens, lengths, cache_keys, cache_values, retention_state, mix_gain,
    query_weight, key_weight, value_weight, out_weight, ffn_gain, routes, route_scores,
    expert_gate, expert_up, expert_down, shared_gate, shared_up, shared_down,
    dense_gate, dense_up, dense_down, dense_mix,
):
    residual, new_keys, new_values = retain(
        tokens, lengths, mix_gain, query_weight, key_weight, value_weight, out_weight,
        cache_keys, cache_values, retention_state,
    )
    normal_ffn = (normed(residual) * ffn_gain).astype(BF)
    layer_out = exchange(
        normal_ffn, residual, routes, route_scores, dense_mix[None, :],
        expert_gate, expert_up, expert_down, shared_gate, shared_up, shared_down,
        dense_gate, dense_up, dense_down,
    )
    return (layer_out, new_keys, new_values)


def solution(mesh):
    row = P("ep", None)
    cube = P("ep", None, None)
    in_specs = (
        row, P("ep"), cube, cube, P("ep", None, None, None), P(), P(), P(), P(), P(), P(),
        row, row, cube, cube, cube, P(), P(), P(), row, row, row, P(),
    )
    return jax.shard_map(
        per_device, mesh=mesh, in_specs=in_specs, out_specs=(row, row, row), check_vma=False
    )
```

```python
import math

import jax
import jax.numpy as jnp
from jax import lax
from jax.experimental import pallas as pl
from jax.experimental.pallas import tpu as pltpu
from jax.sharding import PartitionSpec as P

eps = 1e-06
route_scale = 2.5
rope_base = 10000.0
MESH = pl.DeviceIdType.MESH
BF = jnp.bfloat16
F32 = jnp.float32
scope = jax.named_scope


def normed(values):
    return values * lax.rsqrt(jnp.mean(values * values, axis=-1, keepdims=True) + eps)


def dot(a, b):
    return jnp.dot(a, b, preferred_element_type=F32)


def dot_t(a, b):
    return lax.dot_general(a, b, (((1,), (1,)), ((), ())), preferred_element_type=F32)


def silu(v):
    return v / (1.0 + jnp.exp(-v))


def iota(shape, dim):
    return lax.broadcasted_iota(jnp.int32, shape, dim)


def onehot(mask):
    return jnp.where(mask, 1.0, 0.0).astype(BF)


def sin_cos(angle):
    n = jnp.floor(angle * (2.0 / math.pi) + 0.5)
    r = ((angle - n * 1.5703125) - n * 4.837512969970703125e-4) - n * 7.54978995489188216e-8
    s2 = r * r
    sine = r + r * s2 * ((-1.9515295891e-4 * s2 + 8.3321608736e-3) * s2 - 1.6666654611e-1)
    cosine = 1.0 - 0.5 * s2 + s2 * s2 * (
        (2.443315711809948e-5 * s2 - 1.388731625493765e-3) * s2 + 4.166664568298827e-2
    )
    m = n - 4.0 * jnp.floor(n * 0.25)
    odd = (m == 1.0) | (m == 3.0)
    s_val = jnp.where(odd, cosine, sine)
    c_val = jnp.where(odd, sine, cosine)
    s_val = jnp.where(m >= 2.0, -s_val, s_val)
    c_val = jnp.where((m == 1.0) | (m == 2.0), -c_val, c_val)
    return s_val, c_val


def by_head(wide, rows):
    head = iota((rows, 256), 0) % 8
    total = jnp.zeros((rows, 256), F32)
    for h in range(4):
        total = jnp.where(head == h, wide[:, 256 * h : 256 * h + 256], total)
    return total


def layer_kernel(
    tok_hbm, len_hbm, gain_hbm, fgain_hbm, mix_hbm, routes_hbm, scores_hbm,
    wq_hbm, wk_hbm, wv_hbm, wo_hbm, ck_hbm, cv_hbm, st_hbm,
    eg_hbm, eu_hbm, ed_hbm, sg_hbm, su_hbm, sd_hbm, dg_hbm, du_hbm, dd_hbm,
    out_ref, keys_ref, vals_ref,
    tok_v, len_v, gain_v, fgain_v, mix_v, routes_v, scores_v,
    wq, wk, wv, wo, ck, cv, st,
    eg, eu, ed, sg, su, sd,
    xg, xown, wg, dw, sbuf, rbuf, ybuf, bbuf, pbuf, qbuf, qrows, decay_v, acc_v,
    loc, lw, w_s, w_r, d_s, d_r, x_s, x_r, a_s, a_r, b_s, b_r, p_s, p_r,
):
    me = lax.axis_index("ep")
    q = lax.rem(me, 8)
    p = lax.div(me, 8)
    z = lax.div(p, 4)
    y = lax.rem(p, 4)
    base = me - q

    def mate(k):
        return lax.rem(q + k, 8)

    def plane(dz, dy):
        return lax.rem(z + dz, 4), lax.rem(y + dy, 4)

    def device(zz, yy):
        return (zz * 4 + yy) * 8 + q

    def remote(src, dst, s, r, dev):
        return pltpu.make_async_remote_copy(
            src_ref=src, dst_ref=dst, send_sem=s, recv_sem=r, device_id=(dev,), device_id_type=MESH
        )

    barrier = pltpu.get_barrier_semaphore()
    for k in range(1, 8):
        pl.semaphore_signal(barrier, inc=1, device_id=(base + mate(k),), device_id_type=MESH)
    offsets = [(dz, dy) for dz in (0, 1, 3, 2) for dy in (0, 1, 3, 2) if (dz, dy) != (0, 0)]
    for dz, dy in offsets:
        pl.semaphore_signal(barrier, inc=1, device_id=(device(*plane(dz, dy)),), device_id_type=MESH)

    own = []
    for i, hbm in enumerate((dg_hbm, du_hbm, dd_hbm)):
        for h in range(2):
            own.append(
                pltpu.make_async_copy(
                    hbm.at[pl.ds(16 * h, 16)], dw.at[i, z, y, h], loc.at[2 * i + h]
                )
            )
    fetch = {}

    def want(name, hbm, ref):
        fetch[name] = pltpu.make_async_copy(hbm, ref, lw.at[len(fetch)])

    def ready(*names):
        for name in names:
            fetch[name].wait()

    want("tok", tok_hbm, tok_v)
    want("gain", gain_hbm, gain_v)
    want("len", len_hbm, len_v)
    want("routes", routes_hbm, routes_v)
    want("scores", scores_hbm, scores_v)
    want("wq", wq_hbm, wq)
    want("wk", wk_hbm, wk)
    want("wv", wv_hbm, wv)
    want("ck", ck_hbm, ck)
    for i in range(2):
        want(f"cv{i}", cv_hbm.at[pl.ds(8 * i, 8)], cv.at[pl.ds(8 * i, 8)])
    for i in range(4):
        want(f"st{i}", st_hbm.at[pl.ds(4 * i, 4)], st.at[pl.ds(4 * i, 4)])
    want("wo", wo_hbm, wo)
    want("fgain", fgain_hbm, fgain_v)
    want("sg", sg_hbm, sg)
    want("su", su_hbm, su)
    want("sd", sd_hbm, sd)
    want("eg", eg_hbm.at[0], eg)
    want("eu", eu_hbm.at[0], eu)
    want("ed", ed_hbm.at[0], ed)
    want("mix", mix_hbm, mix_v)
    for c in own:
        c.start()
    for name in fetch:
        fetch[name].start()

    def ring(part, step):
        copies = []
        for half in range(2):
            for sign in range(2):
                away = 1 if sign == 0 else 3
                along_y = (half == 0) == (part == 0)
                dev = device(*(plane(0, away) if along_y else plane(away, 0)))
                back = 0 if step == 0 else (4 - away)
                zz, yy = plane(0, back) if along_y else plane(back, 0)
                cols = pl.ds(0, 1024) if step == 0 else pl.ds(512 * sign, 512)
                if part == 0:
                    block = dw.at[:, zz, yy, half, :, cols]
                elif along_y:
                    block = dw.at[:, :, yy, half, :, cols]
                else:
                    block = dw.at[:, zz, :, half, :, cols]
                i = part * 8 + step * 4 + half * 2 + sign
                copies.append(remote(block, block, d_s.at[i], d_r.at[i], dev))
        return copies

    rings = [ring(0, 0), ring(0, 1), ring(1, 0), ring(1, 1)]

    with scope("route"):
        ready("routes", "scores")
        scores = scores_v[...]
        weight = scores / jnp.sum(scores, axis=0, keepdims=True) * route_scale
        chosen = routes_v[...]
        names = iota((128, 16), 0)
        spread = jnp.zeros((128, 16), F32)
        for k in range(6):
            spread = jnp.where(chosen[k : k + 1, :] == names, weight[k : k + 1, :], spread)
        spread = jnp.concatenate([spread, jnp.zeros((128, 112), F32)], axis=1).T
        wg[q] = spread[:16]

    with scope("qkv"):
        ready("tok", "gain", "len")
        tok = tok_v[...].astype(F32)
        xn = (normed(tok) * gain_v[...]).astype(BF)
        lens = jnp.broadcast_to(len_v[...].astype(F32), (16, 16))
        diag = iota((16, 16), 0) == iota((16, 16), 1)
        len_c = jnp.sum(jnp.where(diag, lens, 0.0), axis=1, keepdims=True)
        fill_c = len_c - 128.0 * jnp.floor(len_c * (1.0 / 128.0))
        lane = iota((16, 128), 1)
        inverse = jnp.exp((lane % 64).astype(F32) * (-math.log(rope_base) / 64.0))
        sine, cosine = sin_cos(len_c * inverse)
        sine = jnp.where(lane < 64, -sine, sine)
        ready("wq", "wk")
        raw_q = dot(xn, wq[...])
        raw_k = dot(xn, wk[...])

        def rotate(raw):
            parts = []
            for h in range(4):
                v = raw[:, 128 * h : 128 * h + 128]
                parts.append(v * cosine + pltpu.roll(v, 64, 1) * sine)
            return jnp.concatenate(parts, axis=1)

        queries = (rotate(raw_q) * 128.0 ** (-0.5)).astype(BF)
        new_keys = rotate(raw_k).astype(BF)
        keys_ref[...] = new_keys
        ready("wv")
        new_values = dot(xn, wv[...]).astype(BF)
        vals_ref[...] = new_values

    with scope("rows"):
        spread_rows = onehot(iota((128, 16), 0) // 8 == iota((128, 16), 1))
        head_512 = iota((128, 512), 0) % 8 == iota((128, 512), 1) // 128
        q_rows = jnp.where(head_512, dot(spread_rows, queries), 0.0)
        own_w = jnp.sum(q_rows * dot(spread_rows, new_keys), axis=-1, keepdims=True)
        own_w = own_w.astype(BF).astype(F32)
        qrows[...] = q_rows
        fill = dot(spread_rows, jnp.broadcast_to(fill_c, (16, 256)).astype(BF))
        row = iota((128, 256), 0)
        col = iota((128, 256), 1)
        head = row % 8
        rate = jnp.full((128, 256), math.log1p(-(2.0 ** -5)), F32)
        for h in range(1, 4):
            rate = jnp.where(head == h, math.log1p(-(2.0 ** (-5 - h))), rate)
        place = (col % 128).astype(F32)
        live = (place < fill) & (col // 128 == (row // 8) % 2)
        decay_v[...] = jnp.where(live, jnp.exp(jnp.maximum(fill - place, 0.0) * rate), 0.0)
        carry = jnp.exp((fill + 1.0) * rate)
        acc_v[...] = own_w * by_head(dot(spread_rows, new_values), 128)

    with scope("barrier"):
        pl.semaphore_wait(barrier, 22)
        w_copies = [
            remote(wg.at[q], wg.at[q], w_s.at[k], w_r.at[k], base + mate(k)) for k in range(1, 8)
        ]
        for c in own:
            c.wait()
        for c in rings[0]:
            c.start()
        for c in w_copies:
            c.start()

    with scope("scores"):
        ready("ck")
        weights = []
        for i in range(8):
            r = slice(16 * i, 16 * i + 16)
            got = dot_t(qrows[r].astype(BF), ck[2 * i : 2 * i + 2].reshape(256, 512))
            weights.append((got * decay_v[r]).astype(BF))

    with scope("ring1"):
        for c in rings[0]:
            c.wait_recv()
        for c in rings[1]:
            c.start()

    with scope("values"):
        for i in range(8):
            if i % 4 == 0:
                ready(f"cv{i // 4}")
            r = slice(16 * i, 16 * i + 16)
            got = dot(weights[i], cv[2 * i : 2 * i + 2].reshape(256, 1024))
            acc_v[r] = acc_v[r] + by_head(got, 16)

    with scope("state"):
        low = iota((16, 512), 0) < 8
        for i in range(8):
            if i % 2 == 0:
                ready(f"st{i // 2}")
            r = slice(16 * i, 16 * i + 16)
            rows = qrows[r]
            both = jnp.concatenate(
                [jnp.where(low, rows, 0.0), jnp.where(low, 0.0, rows)], axis=1
            ).astype(BF)
            got = dot(both, st[2 * i : 2 * i + 2].reshape(1024, 256).astype(BF))
            acc_v[r] = acc_v[r] + got * carry[r]

    with scope("ring2"):
        for c in rings[1]:
            c.wait_recv()
        for c in rings[2]:
            c.start()

    with scope("out"):
        headed = normed(acc_v[...]).astype(BF)
        ready("wo")
        mixed = jnp.zeros((16, 1024), F32)
        for h in range(4):
            pick = onehot(iota((16, 128), 1) == iota((16, 128), 0) * 8 + h)
            mixed = mixed + dot(dot(pick, headed).astype(BF), wo[256 * h : 256 * h + 256])
        residual = tok + normed(mixed)
        ready("fgain")
        xv = (normed(residual) * fgain_v[...]).astype(BF)
        xown[...] = xv
        xg[q] = xv
        x_copies = [
            remote(xown, xg.at[q], x_s.at[k], x_r.at[k], base + mate(k)) for k in range(1, 8)
        ]
        for c in x_copies:
            c.start()

    with scope("shared"):
        ready("sg", "su", "sd")
        hidden = (silu(dot(xv, sg[...])) * dot(xv, su[...])).astype(BF)
        shared = dot(hidden, sd[...])

    with scope("slots"):
        for c in w_copies:
            c.wait_recv()
        w_t = wg[...].reshape(128, 128).T
        before = (iota((128, 128), 0) < iota((128, 128), 1)) & (
            iota((128, 128), 0) // 16 == iota((128, 128), 1) // 16
        )
        rank = dot(onehot(w_t > 0), onehot(before))
        mine = iota((16, 8, 128), 1) == q
        w_p = jnp.sum(jnp.where(mine, w_t.reshape(16, 8, 128), 0.0), axis=1)
        r_p = jnp.sum(jnp.where(mine, rank.reshape(16, 8, 128), 0.0), axis=1)
        slot = iota((16, 16, 128), 1)
        mate_of = iota((16, 16, 128), 2) // 16
        w_b = jnp.broadcast_to(w_p[:, None, :], (16, 16, 128))
        r_b = jnp.broadcast_to(r_p[:, None, :], (16, 16, 128))
        fits = (slot // 2 == mate_of) & (r_b == (slot % 2).astype(F32))
        picked = jnp.where(fits, w_b, 0.0).reshape(256, 128)
        choose = onehot(picked > 0)
        combine = picked.T
        comb_hi = combine.astype(BF)
        comb_lo = (combine - comb_hi.astype(F32)).astype(BF)

    with scope("xwait"):
        for c in x_copies:
            c.wait_recv()
    with scope("send"):
        xall = xg[...].reshape(128, 1024)
        sbuf[...] = dot(choose, xall).astype(BF).reshape(4, 4, 16, 1024)
        out_copies = {}
        for dz, dy in offsets:
            zz, yy = plane(dz, dy)
            i = dz * 4 + dy
            out_copies[i] = remote(
                sbuf.at[zz, yy], rbuf.at[z, y], a_s.at[i], a_r.at[i], device(zz, yy)
            )
            out_copies[i].start()
        rbuf[z, y] = sbuf[z, y]

    with scope("ring3"):
        for c in rings[2]:
            c.wait_recv()
        for c in rings[3]:
            c.start()

    ready("eg", "eu", "ed")
    back_copies = {}
    for dz in (0, 1, 3, 2):
        with scope(f"ewait{dz}"):
            for dy in range(4):
                if (dz, dy) != (0, 0):
                    out_copies[dz * 4 + dy].wait_recv()
        with scope(f"expert{dz}"):
            zz = lax.rem(z + 4 - dz, 4)
            rows = rbuf[zz].reshape(64, 1024)
            hid = (silu(dot(rows, eg[...])) * dot(rows, eu[...])).astype(BF)
            ybuf[zz] = dot(hid, ed[...]).astype(BF).reshape(4, 16, 1024)
            for dy in (0, 1, 3, 2):
                if (dz, dy) != (0, 0):
                    yy = lax.rem(y + 4 - dy, 4)
                    i = dz * 4 + dy
                    back_copies[i] = remote(
                        ybuf.at[zz, yy], bbuf.at[z, y], b_s.at[i], b_r.at[i], device(zz, yy)
                    )
                    back_copies[i].start()
    bbuf[z, y] = ybuf[z, y]

    with scope("dwait"):
        for c in rings[3]:
            c.wait_recv()

    with scope("dense"):
        gate = dot_t(xall, dw[0].reshape(512, 1024))
        up = dot_t(xall, dw[1].reshape(512, 1024))
        dense = dot((silu(gate) * up).astype(BF), dw[2].reshape(512, 1024))
        ready("mix")
        partial = dense * (1.0 / (1.0 + jnp.exp(-mix_v[...])))

    with scope("bwait"):
        for i in back_copies:
            back_copies[i].wait_recv()
    with scope("combine"):
        back = bbuf[...].reshape(256, 1024)
        partial = partial + dot(comb_hi, back) + dot(comb_lo, back)
        pbuf[...] = partial.astype(BF).reshape(8, 16, 1024)
        p_copies = []
        for k in range(1, 8):
            p_copies.append(
                remote(pbuf.at[mate(k)], qbuf.at[q], p_s.at[k], p_r.at[k], base + mate(k))
            )
        for c in p_copies:
            c.start()
        qbuf[q] = pbuf[q]
    with scope("pwait"):
        for c in p_copies:
            c.wait_recv()
    with scope("final"):
        total = shared + jnp.sum(qbuf[...].astype(F32), axis=0)
        out_ref[...] = (residual + normed(total)).astype(BF)

    with scope("drain"):
        for c in w_copies + x_copies + p_copies:
            c.wait_send()
        for r in rings:
            for c in r:
                c.wait_send()
        for group in (out_copies, back_copies):
            for i in group:
                group[i].wait_send()


def per_device(
    tokens, lengths, cache_keys, cache_values, retention_state, mix_gain,
    query_weight, key_weight, value_weight, out_weight, ffn_gain, routes, route_scores,
    expert_gate, expert_up, expert_down, shared_gate, shared_up, shared_down,
    dense_gate, dense_up, dense_down, dense_mix,
):
    vm = pl.BlockSpec(memory_space=pltpu.VMEM)
    hbm = pl.BlockSpec(memory_space=pl.ANY)
    dma = pltpu.SemaphoreType.DMA
    args = (
        tokens, lengths[None, :], mix_gain[None, :], ffn_gain[None, :], dense_mix[None, :],
        routes.T, route_scores.T,
        query_weight, key_weight, value_weight, out_weight,
        cache_keys, cache_values, retention_state.reshape(16, 512, 256),
        expert_gate, expert_up, expert_down, shared_gate, shared_up, shared_down,
        dense_gate, dense_up, dense_down,
    )
    local = [a.shape for a in args[:14]] + [a.shape[-2:] for a in args[14:20]]
    return pl.pallas_call(
        layer_kernel,
        out_shape=(
            jax.ShapeDtypeStruct((16, 1024), BF),
            jax.ShapeDtypeStruct((16, 512), BF),
            jax.ShapeDtypeStruct((16, 1024), BF),
        ),
        in_specs=[hbm] * len(args),
        out_specs=(vm, vm, vm),
        scratch_shapes=[pltpu.VMEM(s, a.dtype) for s, a in zip(local, args)]
        + [
            pltpu.VMEM((8, 16, 1024), BF),
            pltpu.VMEM((16, 1024), BF),
            pltpu.VMEM((8, 16, 128), F32),
            pltpu.VMEM((3, 4, 4, 2, 16, 1024), BF),
            pltpu.VMEM((4, 4, 16, 1024), BF),
            pltpu.VMEM((4, 4, 16, 1024), BF),
            pltpu.VMEM((4, 4, 16, 1024), BF),
            pltpu.VMEM((4, 4, 16, 1024), BF),
            pltpu.VMEM((8, 16, 1024), BF),
            pltpu.VMEM((8, 16, 1024), BF),
            pltpu.VMEM((128, 512), F32),
            pltpu.VMEM((128, 256), F32),
            pltpu.VMEM((128, 256), F32),
            dma((6,)), dma((24,)), dma((8,)), dma((8,)), dma((16,)), dma((16,)),
            dma((8,)), dma((8,)), dma((16,)), dma((16,)), dma((16,)), dma((16,)),
            dma((8,)), dma((8,)),
        ],
        compiler_params=pltpu.CompilerParams(collective_id=0, has_side_effects=True),
    )(*args)


def solution(mesh):
    row = P("ep", None)
    cube = P("ep", None, None)
    in_specs = (
        row, P("ep"), cube, cube, P("ep", None, None, None), P(), P(), P(), P(), P(), P(),
        row, row, cube, cube, cube, P(), P(), P(), row, row, row, P(),
    )
    return jax.shard_map(
        per_device, mesh=mesh, in_specs=in_specs, out_specs=(row, row, row), check_vma=False
    )
```

```python
import math

import jax
import jax.numpy as jnp
from jax import lax
from jax.experimental import pallas as pl
from jax.experimental.pallas import tpu as pltpu
from jax.sharding import PartitionSpec as P

eps = 1e-06
route_scale = 2.5
rope_base = 10000.0
MESH = pl.DeviceIdType.MESH
BF = jnp.bfloat16
F32 = jnp.float32
scope = jax.named_scope


def normed(values):
    return values * lax.rsqrt(jnp.mean(values * values, axis=-1, keepdims=True) + eps)


def dot(a, b):
    return jnp.dot(a, b, preferred_element_type=F32)


def dot_t(a, b):
    return lax.dot_general(a, b, (((1,), (1,)), ((), ())), preferred_element_type=F32)


def silu(v):
    return v / (1.0 + jnp.exp(-v))


def iota(shape, dim):
    return lax.broadcasted_iota(jnp.int32, shape, dim)


def onehot(mask):
    return jnp.where(mask, 1.0, 0.0).astype(BF)


def sin_cos(angle):
    n = jnp.floor(angle * (2.0 / math.pi) + 0.5)
    r = ((angle - n * 1.5703125) - n * 4.837512969970703125e-4) - n * 7.54978995489188216e-8
    s2 = r * r
    sine = r + r * s2 * ((-1.9515295891e-4 * s2 + 8.3321608736e-3) * s2 - 1.6666654611e-1)
    cosine = 1.0 - 0.5 * s2 + s2 * s2 * (
        (2.443315711809948e-5 * s2 - 1.388731625493765e-3) * s2 + 4.166664568298827e-2
    )
    m = n - 4.0 * jnp.floor(n * 0.25)
    odd = (m == 1.0) | (m == 3.0)
    s_val = jnp.where(odd, cosine, sine)
    c_val = jnp.where(odd, sine, cosine)
    s_val = jnp.where(m >= 2.0, -s_val, s_val)
    c_val = jnp.where((m == 1.0) | (m == 2.0), -c_val, c_val)
    return s_val, c_val


def by_head(wide, rows):
    head = iota((rows, 256), 0) % 8
    total = jnp.zeros((rows, 256), F32)
    for h in range(4):
        total = jnp.where(head == h, wide[:, 256 * h : 256 * h + 256], total)
    return total


def layer_kernel(
    tok_hbm, len_hbm, gain_hbm, fgain_hbm, mix_hbm, routes_hbm, scores_hbm,
    wq_hbm, wk_hbm, wv_hbm, wo_hbm, ck_hbm, cv_hbm, st_hbm,
    eg_hbm, eu_hbm, ed_hbm, sg_hbm, su_hbm, sd_hbm, dg_hbm, du_hbm, dd_hbm,
    out_ref, keys_ref, vals_ref,
    tok_v, len_v, gain_v, fgain_v, mix_v, routes_v, scores_v,
    wq, wk, wv, wo, ck, cv, st,
    eg, eu, ed, sg, su, sd,
    xg, xown, wg, wt, dw, dense_v, sbuf, rbuf, ybuf, bbuf, pbuf, qbuf, qrows, decay_v, acc_v,
    loc, lw, w_s, w_r, d_s, d_r, x_s, x_r, a_s, a_r, b_s, b_r, p_s, p_r,
):
    me = lax.axis_index("ep")
    q = lax.rem(me, 8)
    p = lax.div(me, 8)
    z = lax.div(p, 4)
    y = lax.rem(p, 4)
    base = me - q
    other = q + 1 - 2 * lax.rem(q, 2)

    def mate(k):
        return lax.rem(q + k, 8)

    def plane(dz, dy):
        return lax.rem(z + dz, 4), lax.rem(y + dy, 4)

    def device(zz, yy):
        return (zz * 4 + yy) * 8 + q

    def remote(src, dst, s, r, dev):
        return pltpu.make_async_remote_copy(
            src_ref=src, dst_ref=dst, send_sem=s, recv_sem=r, device_id=(dev,), device_id_type=MESH
        )

    barrier = pltpu.get_barrier_semaphore()
    for k in range(1, 8):
        pl.semaphore_signal(barrier, inc=1, device_id=(base + mate(k),), device_id_type=MESH)
    offsets = [(dz, dy) for dz in (0, 1, 3, 2) for dy in (0, 1, 3, 2) if (dz, dy) != (0, 0)]
    for dz, dy in offsets:
        pl.semaphore_signal(barrier, inc=1, device_id=(device(*plane(dz, dy)),), device_id_type=MESH)

    own = []
    for i, hbm in enumerate((dg_hbm, du_hbm, dd_hbm)):
        own.append(pltpu.make_async_copy(hbm, dw.at[i, q], loc.at[i]))
    fetch = {}

    def want(name, hbm, ref):
        fetch[name] = pltpu.make_async_copy(hbm, ref, lw.at[len(fetch)])

    def ready(*names):
        for name in names:
            fetch[name].wait()

    want("tok", tok_hbm, tok_v)
    want("gain", gain_hbm, gain_v)
    want("len", len_hbm, len_v)
    want("routes", routes_hbm, routes_v)
    want("scores", scores_hbm, scores_v)
    want("wq", wq_hbm, wq)
    want("wk", wk_hbm, wk)
    want("wv", wv_hbm, wv)
    want("ck", ck_hbm, ck)
    for i in range(2):
        want(f"cv{i}", cv_hbm.at[pl.ds(8 * i, 8)], cv.at[pl.ds(8 * i, 8)])
    for i in range(4):
        want(f"st{i}", st_hbm.at[pl.ds(4 * i, 4)], st.at[pl.ds(4 * i, 4)])
    want("wo", wo_hbm, wo)
    want("fgain", fgain_hbm, fgain_v)
    want("sg", sg_hbm, sg)
    want("su", su_hbm, su)
    want("sd", sd_hbm, sd)
    want("eg", eg_hbm.at[0], eg)
    want("eu", eu_hbm.at[0], eu)
    want("ed", ed_hbm.at[0], ed)
    want("mix", mix_hbm, mix_v)
    for c in own:
        c.start()
    for name in fetch:
        fetch[name].start()

    def shard(i, which, to):
        block = dw.at[:, which]
        return remote(block, block, d_s.at[i], d_r.at[i], base + to)

    along = [mate(2 * k) for k in range(1, 4)]
    first = [shard(k, q, along[k]) for k in range(3)]
    across = [shard(3, q, other)]
    second = [shard(4 + k, along[k], other) for k in range(3)]

    with scope("route"):
        ready("routes", "scores")
        scores = scores_v[...]
        weight = scores / jnp.sum(scores, axis=0, keepdims=True) * route_scale
        chosen = routes_v[...]
        names = iota((128, 16), 0)
        spread = jnp.zeros((128, 16), F32)
        for k in range(6):
            spread = jnp.where(chosen[k : k + 1, :] == names, weight[k : k + 1, :], spread)
        spread = jnp.concatenate([spread, jnp.zeros((128, 112), F32)], axis=1).T
        wg[z, y] = spread[:16]

    with scope("qkv"):
        ready("tok", "gain", "len")
        tok = tok_v[...].astype(F32)
        xn = (normed(tok) * gain_v[...]).astype(BF)
        lens = jnp.broadcast_to(len_v[...].astype(F32), (16, 16))
        diag = iota((16, 16), 0) == iota((16, 16), 1)
        len_c = jnp.sum(jnp.where(diag, lens, 0.0), axis=1, keepdims=True)
        fill_c = len_c - 128.0 * jnp.floor(len_c * (1.0 / 128.0))
        lane = iota((16, 128), 1)
        inverse = jnp.exp((lane % 64).astype(F32) * (-math.log(rope_base) / 64.0))
        sine, cosine = sin_cos(len_c * inverse)
        sine = jnp.where(lane < 64, -sine, sine)
        ready("wq", "wk")
        raw_q = dot(xn, wq[...])
        raw_k = dot(xn, wk[...])

        def rotate(raw):
            parts = []
            for h in range(4):
                v = raw[:, 128 * h : 128 * h + 128]
                parts.append(v * cosine + pltpu.roll(v, 64, 1) * sine)
            return jnp.concatenate(parts, axis=1)

        queries = (rotate(raw_q) * 128.0 ** (-0.5)).astype(BF)
        new_keys = rotate(raw_k).astype(BF)
        keys_ref[...] = new_keys
        ready("wv")
        new_values = dot(xn, wv[...]).astype(BF)
        vals_ref[...] = new_values

    with scope("rows"):
        spread_rows = onehot(iota((128, 16), 0) // 8 == iota((128, 16), 1))
        head_512 = iota((128, 512), 0) % 8 == iota((128, 512), 1) // 128
        q_rows = jnp.where(head_512, dot(spread_rows, queries), 0.0)
        own_w = jnp.sum(q_rows * dot(spread_rows, new_keys), axis=-1, keepdims=True)
        own_w = own_w.astype(BF).astype(F32)
        qrows[...] = q_rows
        fill = dot(spread_rows, jnp.broadcast_to(fill_c, (16, 256)).astype(BF))
        row = iota((128, 256), 0)
        col = iota((128, 256), 1)
        head = row % 8
        rate = jnp.full((128, 256), math.log1p(-(2.0 ** -5)), F32)
        for h in range(1, 4):
            rate = jnp.where(head == h, math.log1p(-(2.0 ** (-5 - h))), rate)
        place = (col % 128).astype(F32)
        live = (place < fill) & (col // 128 == (row // 8) % 2)
        decay_v[...] = jnp.where(live, jnp.exp(jnp.maximum(fill - place, 0.0) * rate), 0.0)
        carry = jnp.exp((fill + 1.0) * rate)
        acc_v[...] = own_w * by_head(dot(spread_rows, new_values), 128)

    with scope("scores"):
        ready("ck")
        weights = []
        for i in range(8):
            r = slice(16 * i, 16 * i + 16)
            got = dot_t(qrows[r].astype(BF), ck[2 * i : 2 * i + 2].reshape(256, 512))
            weights.append((got * decay_v[r]).astype(BF))

    with scope("values"):
        for i in range(8):
            if i % 4 == 0:
                ready(f"cv{i // 4}")
            r = slice(16 * i, 16 * i + 16)
            got = dot(weights[i], cv[2 * i : 2 * i + 2].reshape(256, 1024))
            acc_v[r] = acc_v[r] + by_head(got, 16)

    with scope("state"):
        low = iota((16, 512), 0) < 8
        for i in range(8):
            if i % 2 == 0:
                ready(f"st{i // 2}")
            r = slice(16 * i, 16 * i + 16)
            rows = qrows[r]
            both = jnp.concatenate(
                [jnp.where(low, rows, 0.0), jnp.where(low, 0.0, rows)], axis=1
            ).astype(BF)
            got = dot(both, st[2 * i : 2 * i + 2].reshape(1024, 256).astype(BF))
            acc_v[r] = acc_v[r] + got * carry[r]

    with scope("barrier"):
        pl.semaphore_wait(barrier, 22)
        w_copies = {}
        for dz, dy in offsets:
            i = dz * 4 + dy
            w_copies[i] = remote(
                wg.at[z, y], wg.at[z, y], w_s.at[i], w_r.at[i], device(*plane(dz, dy))
            )
            w_copies[i].start()
        for c in own:
            c.wait()
        for c in first + across:
            c.start()

    with scope("out"):
        headed = normed(acc_v[...]).astype(BF)
        ready("wo")
        mixed = jnp.zeros((16, 1024), F32)
        for h in range(4):
            pick = onehot(iota((16, 128), 1) == iota((16, 128), 0) * 8 + h)
            mixed = mixed + dot(dot(pick, headed).astype(BF), wo[256 * h : 256 * h + 256])
        residual = tok + normed(mixed)
        ready("fgain")
        xv = (normed(residual) * fgain_v[...]).astype(BF)
        xown[...] = xv
        xg[z, y] = xv
        x_copies = {}
        for dz, dy in offsets:
            i = dz * 4 + dy
            x_copies[i] = remote(xown, xg.at[z, y], x_s.at[i], x_r.at[i], device(*plane(dz, dy)))
            x_copies[i].start()

    with scope("shared"):
        ready("sg", "su", "sd")
        hidden = (silu(dot(xv, sg[...])) * dot(xv, su[...])).astype(BF)
        shared = dot(hidden, sd[...])

    order = (0, 1, 3, 2)
    before = onehot(
        (iota((128, 128), 0) < iota((128, 128), 1))
        & (iota((128, 128), 0) // 16 == iota((128, 128), 1) // 16)
    )
    slot = iota((8, 8, 128), 1)
    sender = iota((8, 8, 128), 2) // 16
    out_copies, picks, rows_of = {}, {}, {}
    for dz in order:
        zz = lax.rem(z + 4 - dz, 4)
        rows_of[dz] = zz
        with scope(f"xwait{dz}"):
            for dy in range(4):
                if (dz, dy) != (0, 0):
                    w_copies[dz * 4 + dy].wait_recv()
                    x_copies[dz * 4 + dy].wait_recv()
        with scope(f"send{dz}"):
            w_all = jnp.concatenate([wg[zz].reshape(64, 128), jnp.zeros((64, 128), F32)], axis=0)
            wt[dz] = w_all.T
            w_p = wt[dz, pl.ds(pl.multiple_of(p * 8, 8), 8), :]
            r_p = dot(onehot(w_p > 0), before)
            w_b = jnp.broadcast_to(w_p[:, None, :], (8, 8, 128))
            r_b = jnp.broadcast_to(r_p[:, None, :], (8, 8, 128))
            fits = (slot // 2 == sender) & (r_b == (slot % 2).astype(F32))
            picked = jnp.where(fits, w_b, 0.0).reshape(64, 128)
            picks[dz] = picked
            choose = onehot(picked > 0)[:, :64]
            sbuf[zz] = dot(choose, xg[zz].reshape(64, 1024)).astype(BF).reshape(8, 8, 1024)
            for k in range(1, 8):
                i = dz * 8 + k
                out_copies[i] = remote(
                    sbuf.at[zz, mate(k)], rbuf.at[zz, q], a_s.at[i], a_r.at[i], base + mate(k)
                )
                out_copies[i].start()
            rbuf[zz, q] = sbuf[zz, q]

    with scope("dfwd"):
        for k in range(3):
            first[k].wait_recv()
            second[2 - k].start()

    ready("eg", "eu", "ed")
    back_copies = {}
    for dz in order:
        zz = rows_of[dz]
        with scope(f"ewait{dz}"):
            for k in range(1, 8):
                out_copies[dz * 8 + k].wait_recv()
        with scope(f"expert{dz}"):
            rows = rbuf[zz].reshape(64, 1024)
            hid = (silu(dot(rows, eg[...])) * dot(rows, eu[...])).astype(BF)
            ybuf[zz] = dot(hid, ed[...]).astype(BF).reshape(8, 8, 1024)
            for k in range(1, 8):
                i = dz * 8 + k
                back_copies[i] = remote(
                    ybuf.at[zz, mate(k)], bbuf.at[zz, q], b_s.at[i], b_r.at[i], base + mate(k)
                )
                back_copies[i].start()
            bbuf[zz, q] = ybuf[zz, q]

    with scope("dwait"):
        for c in across + second:
            c.wait_recv()

    with scope("dense"):
        tokens = xg[...].reshape(256, 1024)
        gate = dot_t(tokens, dw[0].reshape(256, 1024))
        up = dot_t(tokens, dw[1].reshape(256, 1024))
        ready("mix")
        mix = 1.0 / (1.0 + jnp.exp(-mix_v[...]))
        down = dw[2].reshape(256, 1024)
        dense_v[...] = (dot((silu(gate) * up).astype(BF), down) * mix).reshape(4, 64, 1024)

    p_copies = {}
    for dz in order:
        zz = rows_of[dz]
        with scope(f"bwait{dz}"):
            for k in range(1, 8):
                back_copies[dz * 8 + k].wait_recv()
        with scope(f"combine{dz}"):
            combine = picks[dz].T[:64]
            comb_hi = combine.astype(BF)
            comb_lo = (combine - comb_hi.astype(F32)).astype(BF)
            back = bbuf[zz].reshape(64, 1024)
            partial = dense_v[zz] + dot(comb_hi, back) + dot(comb_lo, back)
            pbuf[zz] = partial.astype(BF).reshape(4, 16, 1024)
            for dy in (0, 1, 3, 2):
                if (dz, dy) != (0, 0):
                    yy = lax.rem(y + 4 - dy, 4)
                    i = dz * 4 + dy
                    p_copies[i] = remote(
                        pbuf.at[zz, yy], qbuf.at[z, y], p_s.at[i], p_r.at[i], device(zz, yy)
                    )
                    p_copies[i].start()
    qbuf[z, y] = pbuf[z, y]
    with scope("pwait"):
        for i in p_copies:
            p_copies[i].wait_recv()
    with scope("final"):
        total = shared + jnp.sum(qbuf[...].reshape(16, 16, 1024).astype(F32), axis=0)
        out_ref[...] = (residual + normed(total)).astype(BF)

    with scope("drain"):
        for c in first + across + second:
            c.wait_send()
        for group in (w_copies, x_copies, out_copies, back_copies, p_copies):
            for i in group:
                group[i].wait_send()


def results_kernel(a_in, b_in, c_in, a_out, b_out, c_out, a_v, b_v, c_v, in_s, out_s):
    trio = ((a_in, a_v, a_out), (b_in, b_v, b_out), (c_in, c_v, c_out))
    loads = [pltpu.make_async_copy(i, v, in_s.at[n]) for n, (i, v, _) in enumerate(trio)]
    stores = [pltpu.make_async_copy(v, o, out_s.at[n]) for n, (_, v, o) in enumerate(trio)]
    for c in loads:
        c.start()
    for load, store in zip(loads, stores):
        load.wait()
        store.start()
    for c in stores:
        c.wait()


def per_device(
    tokens, lengths, cache_keys, cache_values, retention_state, mix_gain,
    query_weight, key_weight, value_weight, out_weight, ffn_gain, routes, route_scores,
    expert_gate, expert_up, expert_down, shared_gate, shared_up, shared_down,
    dense_gate, dense_up, dense_down, dense_mix,
):
    vm = pl.BlockSpec(memory_space=pltpu.VMEM)
    hbm = pl.BlockSpec(memory_space=pl.ANY)
    dma = pltpu.SemaphoreType.DMA
    args = (
        tokens, lengths[None, :], mix_gain[None, :], ffn_gain[None, :], dense_mix[None, :],
        routes.T, route_scores.T,
        query_weight, key_weight, value_weight, out_weight,
        cache_keys, cache_values, retention_state.reshape(16, 512, 256),
        expert_gate, expert_up, expert_down, shared_gate, shared_up, shared_down,
        dense_gate, dense_up, dense_down,
    )
    local = [a.shape for a in args[:14]] + [a.shape[-2:] for a in args[14:20]]
    shapes = tuple(jax.ShapeDtypeStruct((16, n), BF) for n in (1024, 512, 1024))
    held = pl.pallas_call(
        layer_kernel,
        out_shape=shapes,
        in_specs=[hbm] * len(args),
        out_specs=(vm, vm, vm),
        scratch_shapes=[pltpu.VMEM(s, a.dtype) for s, a in zip(local, args)]
        + [
            pltpu.VMEM((4, 4, 16, 1024), BF),
            pltpu.VMEM((16, 1024), BF),
            pltpu.VMEM((4, 4, 16, 128), F32),
            pltpu.VMEM((4, 128, 128), F32),
            pltpu.VMEM((3, 8, 32, 1024), BF),
            pltpu.VMEM((4, 64, 1024), F32),
            pltpu.VMEM((4, 8, 8, 1024), BF),
            pltpu.VMEM((4, 8, 8, 1024), BF),
            pltpu.VMEM((4, 8, 8, 1024), BF),
            pltpu.VMEM((4, 8, 8, 1024), BF),
            pltpu.VMEM((4, 4, 16, 1024), BF),
            pltpu.VMEM((4, 4, 16, 1024), BF),
            pltpu.VMEM((128, 512), F32),
            pltpu.VMEM((128, 256), F32),
            pltpu.VMEM((128, 256), F32),
            dma((3,)), dma((24,)), dma((16,)), dma((16,)), dma((8,)), dma((8,)),
            dma((16,)), dma((16,)), dma((32,)), dma((32,)), dma((32,)), dma((32,)),
            dma((16,)), dma((16,)),
        ],
        compiler_params=pltpu.CompilerParams(collective_id=0, has_side_effects=True),
    )(*args)
    return pl.pallas_call(
        results_kernel,
        out_shape=shapes,
        in_specs=[hbm] * 3,
        out_specs=(hbm,) * 3,
        scratch_shapes=[pltpu.VMEM(a.shape, BF) for a in shapes] + [dma((3,)), dma((3,))],
    )(*held)


def solution(mesh):
    row = P("ep", None)
    cube = P("ep", None, None)
    in_specs = (
        row, P("ep"), cube, cube, P("ep", None, None, None), P(), P(), P(), P(), P(), P(),
        row, row, cube, cube, cube, P(), P(), P(), row, row, row, P(),
    )
    return jax.shard_map(
        per_device, mesh=mesh, in_specs=in_specs, out_specs=(row, row, row), check_vma=False
    )
```

```python
import math

import jax
import jax.numpy as jnp
from jax import lax
from jax.experimental import pallas as pl
from jax.experimental.pallas import tpu as pltpu
from jax.sharding import PartitionSpec as P

eps = 1e-06
route_scale = 2.5
rope_base = 10000.0
MESH = pl.DeviceIdType.MESH
BF = jnp.bfloat16
F32 = jnp.float32
scope = jax.named_scope


def normed(values):
    return values * lax.rsqrt(jnp.mean(values * values, axis=-1, keepdims=True) + eps)


def dot(a, b):
    return jnp.dot(a, b, preferred_element_type=F32)


def dot_t(a, b):
    return lax.dot_general(a, b, (((1,), (1,)), ((), ())), preferred_element_type=F32)


def silu(v):
    return v / (1.0 + jnp.exp(-v))


def iota(shape, dim):
    return lax.broadcasted_iota(jnp.int32, shape, dim)


def onehot(mask):
    return jnp.where(mask, 1.0, 0.0).astype(BF)


def sin_cos(angle):
    n = jnp.floor(angle * (2.0 / math.pi) + 0.5)
    r = ((angle - n * 1.5703125) - n * 4.837512969970703125e-4) - n * 7.54978995489188216e-8
    s2 = r * r
    sine = r + r * s2 * ((-1.9515295891e-4 * s2 + 8.3321608736e-3) * s2 - 1.6666654611e-1)
    cosine = 1.0 - 0.5 * s2 + s2 * s2 * (
        (2.443315711809948e-5 * s2 - 1.388731625493765e-3) * s2 + 4.166664568298827e-2
    )
    m = n - 4.0 * jnp.floor(n * 0.25)
    odd = (m == 1.0) | (m == 3.0)
    s_val = jnp.where(odd, cosine, sine)
    c_val = jnp.where(odd, sine, cosine)
    s_val = jnp.where(m >= 2.0, -s_val, s_val)
    c_val = jnp.where((m == 1.0) | (m == 2.0), -c_val, c_val)
    return s_val, c_val


def by_head(wide, rows):
    head = iota((rows, 256), 0) % 8
    total = jnp.zeros((rows, 256), F32)
    for h in range(4):
        total = jnp.where(head == h, wide[:, 256 * h : 256 * h + 256], total)
    return total


def layer_kernel(
    tok_hbm, len_hbm, gain_hbm, fgain_hbm, mix_hbm, routes_hbm, scores_hbm,
    wq_hbm, wk_hbm, wv_hbm, wo_hbm, ck_hbm, cv_hbm, st_hbm,
    eg_hbm, eu_hbm, ed_hbm, sg_hbm, su_hbm, sd_hbm, dg_hbm, du_hbm, dd_hbm,
    out_ref, keys_hbm, vals_hbm,
    tok_v, len_v, gain_v, fgain_v, mix_v, routes_v, scores_v,
    wq, wk, wv, wo, ck, cv, st,
    eg, eu, ed, sg, su, sd,
    xg, xown, wg, wown, keys_v, vals_v, dw, dense_v, sbuf, rbuf, ybuf, bbuf, pbuf, qbuf, qrows, decay_v, acc_v,
    loc, lw, w_s, w_r, d_s, d_r, x_s, x_r, a_s, a_r, b_s, b_r, p_s, p_r,
):
    me = lax.axis_index("ep")
    core = lax.rem(me, 2)
    x = lax.rem(lax.div(me, 2), 4)
    y = lax.rem(lax.div(me, 8), 4)
    z = lax.div(me, 32)
    xp, yp = lax.div(x, 2), lax.div(y, 2)
    xq, yq = x + xp * (3 - 2 * x), y + yp * (3 - 2 * y)
    q = yq * 4 + xq * 2 + core
    t = yp * 2 + xp
    p = z * 4 + t

    def at(zz, tt, qq):
        x_half, y_half = lax.rem(tt, 2), lax.div(tt, 2)
        x_in, y_in = lax.rem(lax.div(qq, 2), 2), lax.div(qq, 4)
        x_at = x_in + x_half * (3 - 2 * x_in)
        y_at = y_in + y_half * (3 - 2 * y_in)
        return zz * 32 + y_at * 8 + x_at * 2 + lax.rem(qq, 2)

    def near(qq):
        return at(z, t, qq)

    other = q + 1 - 2 * core

    def mate(k):
        return lax.rem(q + k, 8)

    def plane(dz, dt):
        return lax.rem(z + dz, 4), lax.rem(t + dt, 4)

    def experts_of(which):
        return pl.ds(pl.multiple_of(which * 8, 8), 8)

    def device(zz, tt):
        return at(zz, tt, q)

    def remote(src, dst, s, r, dev):
        return pltpu.make_async_remote_copy(
            src_ref=src, dst_ref=dst, send_sem=s, recv_sem=r, device_id=(dev,), device_id_type=MESH
        )

    barrier = pltpu.get_barrier_semaphore()
    for k in range(1, 8):
        pl.semaphore_signal(barrier, inc=1, device_id=(near(mate(k)),), device_id_type=MESH)
    offsets = [(dz, dy) for dz in (2, 0, 1, 3) for dy in (0, 1, 2, 3) if (dz, dy) != (0, 0)]
    for dz, dy in offsets:
        pl.semaphore_signal(barrier, inc=1, device_id=(device(*plane(dz, dy)),), device_id_type=MESH)

    own = []
    for i, hbm in enumerate((dg_hbm, du_hbm, dd_hbm)):
        own.append(pltpu.make_async_copy(hbm, dw.at[i, q], loc.at[0]))
    results = (
        pltpu.make_async_copy(keys_v, keys_hbm, loc.at[1]),
        pltpu.make_async_copy(vals_v, vals_hbm, loc.at[2]),
    )
    fetch = {}

    sems = []

    def want(name, hbm, ref, group=None):
        if group is None or group not in sems:
            sems.append(group)
        slot = len(sems) - 1 if group is None else sems.index(group)
        fetch[name] = pltpu.make_async_copy(hbm, ref, lw.at[slot])

    def ready(*names):
        for name in names:
            fetch[name].wait()

    def ready_all(group, ref):
        pltpu.make_async_copy(ref, ref, lw.at[sems.index(group)]).wait()

    def begin(*names):
        for name in names:
            fetch[name].start()

    want("tok", tok_hbm, tok_v)
    want("gain", gain_hbm, gain_v)
    want("len", len_hbm, len_v)
    want("routes", routes_hbm, routes_v)
    want("scores", scores_hbm, scores_v)
    want("wq", wq_hbm, wq, "qk")
    want("wk", wk_hbm, wk, "qk")
    want("wv", wv_hbm, wv)
    want("ck", ck_hbm, ck)
    for i in range(2):
        want(f"cv{i}", cv_hbm.at[pl.ds(8 * i, 8)], cv.at[pl.ds(8 * i, 8)])
    for i in range(4):
        want(f"st{i}", st_hbm.at[pl.ds(4 * i, 4)], st.at[pl.ds(4 * i, 4)])
    want("wo", wo_hbm, wo)
    want("fgain", fgain_hbm, fgain_v)
    want("sg", sg_hbm, sg, "shared")
    want("su", su_hbm, su, "shared")
    want("sd", sd_hbm, sd, "shared")
    want("eg", eg_hbm.at[0], eg, "expert")
    want("eu", eu_hbm.at[0], eu, "expert")
    want("ed", ed_hbm.at[0], ed, "expert")
    want("mix", mix_hbm, mix_v)
    for c in own:
        c.start()
    begin("tok", "gain", "len", "routes", "scores", "wq", "wk", "wv")

    up, down = q + 2 - 4 * xq, mate(4)
    far = lax.rem(up + 4, 8)

    def shard(group, which, to, cols=slice(None)):
        block = dw.at[:, which, :, cols]
        return remote(block, block, d_s.at[0], d_r.at[group], near(to))

    def arrived(ref, sem):
        remote(ref, ref, d_s.at[0], sem, near(other)).wait_recv()

    def gone(ref, sem):
        remote(ref, ref, sem, d_r.at[0], near(other)).wait_send()

    first = [shard(0, q, up), shard(0, q, down)]
    second = [shard(1, up, down, pl.ds(0, 512)), shard(1, down, up, pl.ds(512, 512))]
    across = shard(2, q, other)
    handed = [shard(2, down, other), shard(2, up, other)]
    third = shard(2, far, other)

    with scope("route"):
        ready("routes", "scores")
        scores = scores_v[...]
        weight = scores / jnp.sum(scores, axis=0, keepdims=True) * route_scale
        names = routes_v[...]
        halves = ((names >> 4) & 1) * 2 + ((names >> 2) & 1)
        x_in = ((names >> 1) & 1) ^ ((names >> 2) & 1)
        y_in = ((names >> 3) & 1) ^ ((names >> 4) & 1)
        chosen = (names >> 5) * 32 + halves * 8 + y_in * 4 + x_in * 2 + (names & 1)
        names = iota((128, 16), 0)
        spread = jnp.zeros((128, 16), F32)
        for k in range(6):
            spread = jnp.where(chosen[k : k + 1, :] == names, weight[k : k + 1, :], spread)
        wown[...] = jnp.concatenate([spread, jnp.zeros((128, 112), F32)], axis=1)
        wg[z, t] = wown[experts_of(p), :]

    begin("ck", "cv0", "cv1")
    with scope("qkv"):
        ready("tok", "gain", "len")
        tok = tok_v[...].astype(F32)
        xn = (normed(tok) * gain_v[...]).astype(BF)
        lens = jnp.broadcast_to(len_v[...].astype(F32), (16, 16))
        diag = iota((16, 16), 0) == iota((16, 16), 1)
        len_c = jnp.sum(jnp.where(diag, lens, 0.0), axis=1, keepdims=True)
        fill_c = len_c - 128.0 * jnp.floor(len_c * (1.0 / 128.0))
        lane = iota((16, 128), 1)
        inverse = jnp.exp((lane % 64).astype(F32) * (-math.log(rope_base) / 64.0))
        sine, cosine = sin_cos(len_c * inverse)
        sine = jnp.where(lane < 64, -sine, sine)
        ready_all("qk", ck)
        raw_q = dot(xn, wq[...])
        raw_k = dot(xn, wk[...])

        def rotate(raw):
            parts = []
            for h in range(4):
                v = raw[:, 128 * h : 128 * h + 128]
                parts.append(v * cosine + pltpu.roll(v, 64, 1) * sine)
            return jnp.concatenate(parts, axis=1)

        queries = (rotate(raw_q) * 128.0 ** (-0.5)).astype(BF)
        new_keys = rotate(raw_k).astype(BF)
        keys_v[...] = new_keys
        results[0].start()
        ready("wv")
        new_values = dot(xn, wv[...]).astype(BF)
        vals_v[...] = new_values
        results[1].start()

    begin("st0", "st1", "st2", "st3", "wo", "fgain")
    with scope("rows"):
        spread_rows = onehot(iota((128, 16), 0) // 8 == iota((128, 16), 1))
        head_512 = iota((128, 512), 0) % 8 == iota((128, 512), 1) // 128
        q_rows = jnp.where(head_512, dot(spread_rows, queries), 0.0)
        own_w = jnp.sum(q_rows * dot(spread_rows, new_keys), axis=-1, keepdims=True)
        own_w = own_w.astype(BF).astype(F32)
        qrows[...] = q_rows
        fill = dot(spread_rows, jnp.broadcast_to(fill_c, (16, 256)).astype(BF))
        row = iota((128, 256), 0)
        col = iota((128, 256), 1)
        head = row % 8
        rate = jnp.full((128, 256), math.log1p(-(2.0 ** -5)), F32)
        for h in range(1, 4):
            rate = jnp.where(head == h, math.log1p(-(2.0 ** (-5 - h))), rate)
        place = (col % 128).astype(F32)
        live = (place < fill) & (col // 128 == (row // 8) % 2)
        decay_v[...] = jnp.where(live, jnp.exp(jnp.maximum(fill - place, 0.0) * rate), 0.0)
        carry = jnp.exp((fill + 1.0) * rate)
        acc_v[...] = own_w * by_head(dot(spread_rows, new_values), 128)

    with scope("scores"):
        ready("ck")
        weights = []
        for i in range(8):
            r = slice(16 * i, 16 * i + 16)
            got = dot_t(qrows[r].astype(BF), ck[2 * i : 2 * i + 2].reshape(256, 512))
            weights.append((got * decay_v[r]).astype(BF))

    begin("sg", "su", "sd", "eg", "eu", "ed", "mix")
    with scope("values"):
        for i in range(8):
            if i % 4 == 0:
                ready(f"cv{i // 4}")
            r = slice(16 * i, 16 * i + 16)
            got = dot(weights[i], cv[2 * i : 2 * i + 2].reshape(256, 1024))
            acc_v[r] = acc_v[r] + by_head(got, 16)

    with scope("barrier"):
        pl.semaphore_wait(barrier, 22)
    with scope("early"):
        for dz, dy in offsets:
            zz, tt = plane(dz, dy)
            mine = wown.at[experts_of(zz * 4 + tt), :]
            remote(mine, wg.at[z, t], w_s.at[0], w_r.at[dz], device(zz, tt)).start()
        pltpu.make_async_copy(dw.at[:, q], dw.at[:, q], loc.at[0]).wait()
        for c in first:
            c.start()
        across.start()

    with scope("state"):
        low = iota((16, 512), 0) < 8
        for i in range(8):
            if i % 2 == 0:
                ready(f"st{i // 2}")
            r = slice(16 * i, 16 * i + 16)
            rows = qrows[r]
            both = jnp.concatenate(
                [jnp.where(low, rows, 0.0), jnp.where(low, 0.0, rows)], axis=1
            ).astype(BF)
            got = dot(both, st[2 * i : 2 * i + 2].reshape(1024, 256).astype(BF))
            acc_v[r] = acc_v[r] + got * carry[r]

    with scope("out"):
        headed = normed(acc_v[...]).astype(BF)
        ready("wo")
        mixed = jnp.zeros((16, 1024), F32)
        for h in range(4):
            pick = onehot(iota((16, 128), 1) == iota((16, 128), 0) * 8 + h)
            mixed = mixed + dot(dot(pick, headed).astype(BF), wo[256 * h : 256 * h + 256])
        residual = tok + normed(mixed)
        ready("fgain")
        xv = (normed(residual) * fgain_v[...]).astype(BF)
        xown[...] = xv
        xg[z, t] = xv
        for dz, dy in offsets:
            dev = device(*plane(dz, dy))
            remote(xown, xg.at[z, t], x_s.at[0], x_r.at[dz], dev).start()

    with scope("shared"):
        ready_all("shared", dw)
        hidden = (silu(dot(xv, sg[...])) * dot(xv, su[...])).astype(BF)
        shared = dot(hidden, sd[...])

    with scope("pump1"):
        arrived(dw.at[:, pl.ds(0, 2)], d_r.at[0])
        for c in second + handed:
            c.start()

    before = onehot(
        (iota((128, 128), 0) < iota((128, 128), 1))
        & (iota((128, 128), 0) // 16 == iota((128, 128), 1) // 16)
    )
    slot = iota((8, 8, 128), 1)
    sender = iota((8, 8, 128), 2) // 16
    picks = {}

    def row_at(dz):
        return lax.rem(z + 4 - dz, 4)

    def dispatch(dz):
        zz = row_at(dz)
        with scope(f"xwait{dz}"):
            count = pl.ds(0, 3 if dz == 0 else 4)
            arrived(wg.at[zz, count], w_r.at[dz])
            arrived(xg.at[zz, count], x_r.at[dz])
        with scope(f"send{dz}"):
            w_p = wg[zz, 0]
            for d in range(1, 4):
                w_p = w_p + pltpu.roll(wg[zz, d], 16 * d, 1)
            r_p = dot(onehot(w_p > 0), before)
            w_b = jnp.broadcast_to(w_p[:, None, :], (8, 8, 128))
            r_b = jnp.broadcast_to(r_p[:, None, :], (8, 8, 128))
            fits = (slot // 2 == sender) & (r_b == (slot % 2).astype(F32))
            picked = jnp.where(fits, w_b, 0.0).reshape(64, 128)
            picks[dz] = picked
            choose = onehot(picked > 0)[:, :64]
            sbuf[zz] = dot(choose, xg[zz].reshape(64, 1024)).astype(BF).reshape(8, 8, 1024)
            for k in range(1, 8):
                to = mate(k)
                remote(sbuf.at[zz, to], rbuf.at[zz, q], a_s.at[0], a_r.at[dz], near(to)).start()
            rbuf[zz, q] = sbuf[zz, q]

    def expert(dz):
        zz = row_at(dz)
        with scope(f"ewait{dz}"):
            arrived(rbuf.at[zz, pl.ds(0, 7)], a_r.at[dz])
        with scope(f"expert{dz}"):
            rows = rbuf[zz].reshape(64, 1024)
            hid = (silu(dot(rows, eg[...])) * dot(rows, eu[...])).astype(BF)
            ybuf[zz] = dot(hid, ed[...]).astype(BF).reshape(8, 8, 1024)
            for k in range(1, 8):
                to = mate(k)
                remote(ybuf.at[zz, to], bbuf.at[zz, q], b_s.at[0], b_r.at[dz], near(to)).start()
            bbuf[zz, q] = ybuf[zz, q]

    def gather(dz):
        zz = row_at(dz)
        with scope(f"bwait{dz}"):
            arrived(bbuf.at[zz, pl.ds(0, 7)], b_r.at[dz])
        with scope(f"combine{dz}"):
            combine = picks[dz].T[:64]
            comb_hi = combine.astype(BF)
            comb_lo = (combine - comb_hi.astype(F32)).astype(BF)
            back = bbuf[zz].reshape(64, 1024)
            partial = dense_v[zz] + dot(comb_hi, back) + dot(comb_lo, back)
            pbuf[zz] = partial.astype(BF).reshape(4, 16, 1024)
            for dy in (2, 1, 3, 0):
                if (dz, dy) != (0, 0):
                    tt = lax.rem(t + 4 - dy, 4)
                    sums = pbuf.at[zz, tt]
                    remote(sums, qbuf.at[p], p_s.at[0], p_r.at[0], device(zz, tt)).start()

    dispatch(0)
    dispatch(2)
    dispatch(1)
    ready_all("expert", dw)
    expert(0)
    dispatch(3)
    with scope("pump2"):
        arrived(dw.at[:, 0], d_r.at[1])
        third.start()
    expert(2)
    with scope("dwait"):
        arrived(dw.at[:, pl.ds(0, 4)], d_r.at[2])
    with scope("dense"):
        tokens = xg[...].reshape(256, 1024)
        gate = dot_t(tokens, dw[0].reshape(256, 1024))
        raised = dot_t(tokens, dw[1].reshape(256, 1024))
        ready("mix")
        mix = 1.0 / (1.0 + jnp.exp(-mix_v[...]))
        lowered = dot((silu(gate) * raised).astype(BF), dw[2].reshape(256, 1024))
        dense_v[...] = (lowered * mix).reshape(4, 64, 1024)
    expert(1)
    expert(3)
    gather(0)
    gather(2)
    gather(1)
    gather(3)
    qbuf[p] = pbuf[z, t]
    with scope("pwait"):
        arrived(qbuf.at[pl.ds(0, 15)], p_r.at[0])
    with scope("final"):
        total = shared + jnp.sum(qbuf[...].astype(F32), axis=0)
        out_ref[...] = (residual + normed(total)).astype(BF)

    with scope("drain"):
        for c in results:
            c.wait()
        gone(dw.at[:, pl.ds(0, 7)], d_s.at[0])
        gone(wown.at[pl.ds(0, 120), :], w_s.at[0])
        gone(qbuf.at[pl.ds(0, 15)], x_s.at[0])
        gone(sbuf.at[:, pl.ds(0, 7)], a_s.at[0])
        gone(ybuf.at[:, pl.ds(0, 7)], b_s.at[0])
        gone(qbuf.at[pl.ds(0, 15)], p_s.at[0])


def results_kernel(a_in, b_in, c_in, a_out, b_out, c_out, a_v, b_v, c_v, in_s, out_s):
    trio = ((a_in, a_v, a_out), (b_in, b_v, b_out), (c_in, c_v, c_out))
    loads = [pltpu.make_async_copy(i, v, in_s.at[n]) for n, (i, v, _) in enumerate(trio)]
    stores = [pltpu.make_async_copy(v, o, out_s.at[n]) for n, (_, v, o) in enumerate(trio)]
    for c in loads:
        c.start()
    for load, store in zip(loads, stores):
        load.wait()
        store.start()
    for c in stores:
        c.wait()


def per_device(
    tokens, lengths, cache_keys, cache_values, retention_state, mix_gain,
    query_weight, key_weight, value_weight, out_weight, ffn_gain, routes, route_scores,
    expert_gate, expert_up, expert_down, shared_gate, shared_up, shared_down,
    dense_gate, dense_up, dense_down, dense_mix,
):
    vm = pl.BlockSpec(memory_space=pltpu.VMEM)
    hbm = pl.BlockSpec(memory_space=pl.ANY)
    dma = pltpu.SemaphoreType.DMA
    args = (
        tokens, lengths[None, :], mix_gain[None, :], ffn_gain[None, :], dense_mix[None, :],
        routes.T, route_scores.T,
        query_weight, key_weight, value_weight, out_weight,
        cache_keys, cache_values, retention_state.reshape(16, 512, 256),
        expert_gate, expert_up, expert_down, shared_gate, shared_up, shared_down,
        dense_gate, dense_up, dense_down,
    )
    local = [a.shape for a in args[:14]] + [a.shape[-2:] for a in args[14:20]]
    shapes = tuple(jax.ShapeDtypeStruct((16, n), BF) for n in (1024, 512, 1024))
    held = pl.pallas_call(
        layer_kernel,
        out_shape=shapes,
        in_specs=[hbm] * len(args),
        out_specs=(vm, hbm, hbm),
        scratch_shapes=[pltpu.VMEM(s, a.dtype) for s, a in zip(local, args)]
        + [
            pltpu.VMEM((4, 4, 16, 1024), BF),
            pltpu.VMEM((16, 1024), BF),
            pltpu.VMEM((4, 4, 8, 128), F32),
            pltpu.VMEM((128, 128), F32),
            pltpu.VMEM((16, 512), BF),
            pltpu.VMEM((16, 1024), BF),
            pltpu.VMEM((3, 8, 32, 1024), BF),
            pltpu.VMEM((4, 64, 1024), F32),
            pltpu.VMEM((4, 8, 8, 1024), BF),
            pltpu.VMEM((4, 8, 8, 1024), BF),
            pltpu.VMEM((4, 8, 8, 1024), BF),
            pltpu.VMEM((4, 8, 8, 1024), BF),
            pltpu.VMEM((4, 4, 16, 1024), BF),
            pltpu.VMEM((16, 16, 1024), BF),
            pltpu.VMEM((128, 512), F32),
            pltpu.VMEM((128, 256), F32),
            pltpu.VMEM((128, 256), F32),
            dma((3,)), dma((19,)), dma((1,)), dma((4,)), dma((1,)), dma((3,)),
            dma((1,)), dma((4,)), dma((1,)), dma((4,)), dma((1,)), dma((4,)),
            dma((1,)), dma((1,)),
        ],
        compiler_params=pltpu.CompilerParams(collective_id=0, has_side_effects=True),
    )(*args)
    return pl.pallas_call(
        results_kernel,
        out_shape=shapes,
        in_specs=[hbm] * 3,
        out_specs=(hbm,) * 3,
        scratch_shapes=[pltpu.VMEM(a.shape, BF) for a in shapes] + [dma((3,)), dma((3,))],
    )(*held)


def solution(mesh):
    row = P("ep", None)
    cube = P("ep", None, None)
    in_specs = (
        row, P("ep"), cube, cube, P("ep", None, None, None), P(), P(), P(), P(), P(), P(),
        row, row, cube, cube, cube, P(), P(), P(), row, row, row, P(),
    )
    return jax.shard_map(
        per_device, mesh=mesh, in_specs=in_specs, out_specs=(row, row, row), check_vma=False
    )
```

```python
import math

import jax
import jax.numpy as jnp
from jax import lax
from jax.experimental import pallas as pl
from jax.experimental.pallas import tpu as pltpu
from jax.sharding import PartitionSpec as P

eps = 1e-06
route_scale = 2.5
rope_base = 10000.0
MESH = pl.DeviceIdType.MESH
BF = jnp.bfloat16
F32 = jnp.float32
scope = jax.named_scope


def normed(values):
    return values * lax.rsqrt(jnp.mean(values * values, axis=-1, keepdims=True) + eps)


def dot(a, b):
    return jnp.dot(a, b, preferred_element_type=F32)


def dot_t(a, b):
    return lax.dot_general(a, b, (((1,), (1,)), ((), ())), preferred_element_type=F32)


def silu(v):
    return v / (1.0 + jnp.exp(-v))


def iota(shape, dim):
    return lax.broadcasted_iota(jnp.int32, shape, dim)


def onehot(mask):
    return jnp.where(mask, 1.0, 0.0).astype(BF)


def sin_cos(angle):
    n = jnp.floor(angle * (2.0 / math.pi) + 0.5)
    r = ((angle - n * 1.5703125) - n * 4.837512969970703125e-4) - n * 7.54978995489188216e-8
    s2 = r * r
    sine = r + r * s2 * ((-1.9515295891e-4 * s2 + 8.3321608736e-3) * s2 - 1.6666654611e-1)
    cosine = 1.0 - 0.5 * s2 + s2 * s2 * (
        (2.443315711809948e-5 * s2 - 1.388731625493765e-3) * s2 + 4.166664568298827e-2
    )
    m = n - 4.0 * jnp.floor(n * 0.25)
    odd = (m == 1.0) | (m == 3.0)
    s_val = jnp.where(odd, cosine, sine)
    c_val = jnp.where(odd, sine, cosine)
    s_val = jnp.where(m >= 2.0, -s_val, s_val)
    c_val = jnp.where((m == 1.0) | (m == 2.0), -c_val, c_val)
    return s_val, c_val


def by_head(wide, rows):
    head = iota((rows, 256), 0) % 8
    total = jnp.zeros((rows, 256), F32)
    for h in range(4):
        total = jnp.where(head == h, wide[:, 256 * h : 256 * h + 256], total)
    return total


def layer_kernel(
    tok_hbm, len_hbm, gain_hbm, fgain_hbm, mix_hbm, routes_hbm, scores_hbm,
    wq_hbm, wk_hbm, wv_hbm, wo_hbm, ck_hbm, cv_hbm, st_hbm,
    eg_hbm, eu_hbm, ed_hbm, sg_hbm, su_hbm, sd_hbm, dg_hbm, du_hbm, dd_hbm,
    out_ref, keys_hbm, vals_hbm,
    tok_v, len_v, gain_v, fgain_v, mix_v, routes_v, scores_v,
    wq, wk, wv, wo, ck, cv, st,
    eg, eu, ed, sg, su, sd,
    xg, xown, wg, wown, keys_v, vals_v, dw, dense_v, sbuf, rbuf, ybuf, bbuf, pbuf, qbuf, qrows, decay_v, acc_v,
    loc, lw, w_s, w_r, d_s, d_r, x_s, x_r, a_s, a_r, b_s, b_r, p_s, p_r,
):
    me = lax.axis_index("ep")
    core = lax.rem(me, 2)
    x = lax.rem(lax.div(me, 2), 4)
    y = lax.rem(lax.div(me, 8), 4)
    z = lax.div(me, 32)
    xp, yp = lax.div(x, 2), lax.div(y, 2)
    xq, yq = x + xp * (3 - 2 * x), y + yp * (3 - 2 * y)
    q = yq * 4 + xq * 2 + core
    t = yp * 2 + xp
    p = z * 4 + t

    def at(zz, tt, qq):
        x_half, y_half = lax.rem(tt, 2), lax.div(tt, 2)
        x_in, y_in = lax.rem(lax.div(qq, 2), 2), lax.div(qq, 4)
        x_at = x_in + x_half * (3 - 2 * x_in)
        y_at = y_in + y_half * (3 - 2 * y_in)
        return zz * 32 + y_at * 8 + x_at * 2 + lax.rem(qq, 2)

    def near(qq):
        return at(z, t, qq)

    other = q + 1 - 2 * core

    def mate(k):
        return lax.rem(q + k, 8)

    def plane(dz, dt):
        return lax.rem(z + dz, 4), lax.rem(t + dt, 4)

    def experts_of(which):
        return pl.ds(pl.multiple_of(which * 8, 8), 8)

    def device(zz, tt):
        return at(zz, tt, q)

    def remote(src, dst, s, r, dev):
        return pltpu.make_async_remote_copy(
            src_ref=src, dst_ref=dst, send_sem=s, recv_sem=r, device_id=(dev,), device_id_type=MESH
        )

    barrier = pltpu.get_barrier_semaphore()
    for k in range(1, 8):
        pl.semaphore_signal(barrier, inc=1, device_id=(near(mate(k)),), device_id_type=MESH)
    offsets = [(dz, dy) for dz in (2, 0, 1, 3) for dy in (0, 1, 2, 3) if (dz, dy) != (0, 0)]
    for dz, dy in offsets:
        pl.semaphore_signal(barrier, inc=1, device_id=(device(*plane(dz, dy)),), device_id_type=MESH)

    own = []
    for i, hbm in enumerate((dg_hbm, du_hbm, dd_hbm)):
        own.append(pltpu.make_async_copy(hbm, dw.at[i, q], loc.at[0]))
    results = (
        pltpu.make_async_copy(keys_v, keys_hbm, loc.at[1]),
        pltpu.make_async_copy(vals_v, vals_hbm, loc.at[2]),
    )
    fetch = {}

    sems = []

    def want(name, hbm, ref, group=None):
        if group is None or group not in sems:
            sems.append(group)
        slot = len(sems) - 1 if group is None else sems.index(group)
        fetch[name] = pltpu.make_async_copy(hbm, ref, lw.at[slot])

    def ready(*names):
        for name in names:
            fetch[name].wait()

    def ready_all(group, ref):
        pltpu.make_async_copy(ref, ref, lw.at[sems.index(group)]).wait()

    def begin(*names):
        for name in names:
            fetch[name].start()

    want("tok", tok_hbm, tok_v)
    want("gain", gain_hbm, gain_v)
    want("len", len_hbm, len_v)
    want("routes", routes_hbm, routes_v)
    want("scores", scores_hbm, scores_v)
    want("wq", wq_hbm, wq, "qk")
    want("wk", wk_hbm, wk, "qk")
    want("wv", wv_hbm, wv)
    want("ck", ck_hbm, ck)
    for i in range(2):
        want(f"cv{i}", cv_hbm.at[pl.ds(8 * i, 8)], cv.at[pl.ds(8 * i, 8)])
    for i in range(4):
        want(f"st{i}", st_hbm.at[pl.ds(4 * i, 4)], st.at[pl.ds(4 * i, 4)])
    want("wo", wo_hbm, wo)
    want("fgain", fgain_hbm, fgain_v)
    want("sg", sg_hbm, sg, "shared")
    want("su", su_hbm, su, "shared")
    want("sd", sd_hbm, sd, "shared")
    want("eg", eg_hbm.at[0], eg, "expert")
    want("eu", eu_hbm.at[0], eu, "expert")
    want("ed", ed_hbm.at[0], ed, "expert")
    want("mix", mix_hbm, mix_v)
    for c in own:
        c.start()
    begin("tok", "gain", "len", "routes", "scores", "wq", "wk", "wv")

    up, down = q + 2 - 4 * xq, mate(4)
    far = lax.rem(up + 4, 8)

    turn = 1 - 2 * core
    reach = (up + turn, down + turn, far + turn, far, down, up, other)

    def shard(group, which, to, cols=slice(None)):
        block = dw.at[:, which, :, cols]
        return remote(block, block, d_s.at[0], d_r.at[group], near(to))

    def arrived(ref, sem):
        remote(ref, ref, d_s.at[0], sem, near(other)).wait_recv()

    def gone(ref, sem):
        remote(ref, ref, sem, d_r.at[0], near(other)).wait_send()

    first = [shard(0, q, up), shard(0, q, down)]
    second = [shard(1, up, down, pl.ds(0, 512)), shard(1, down, up, pl.ds(512, 512))]
    across = shard(2, q, other)
    handed = [shard(2, down, other), shard(2, up, other)]
    third = shard(2, far, other)

    with scope("route"):
        ready("routes", "scores")
        scores = scores_v[...]
        weight = scores / jnp.sum(scores, axis=0, keepdims=True) * route_scale
        names = routes_v[...]
        halves = ((names >> 4) & 1) * 2 + ((names >> 2) & 1)
        x_in = ((names >> 1) & 1) ^ ((names >> 2) & 1)
        y_in = ((names >> 3) & 1) ^ ((names >> 4) & 1)
        chosen = (names >> 5) * 32 + halves * 8 + y_in * 4 + x_in * 2 + (names & 1)
        names = iota((128, 16), 0)
        spread = jnp.zeros((128, 16), F32)
        for k in range(6):
            spread = jnp.where(chosen[k : k + 1, :] == names, weight[k : k + 1, :], spread)
        wown[...] = jnp.concatenate([spread, jnp.zeros((128, 112), F32)], axis=1)
        wg[z, t] = wown[experts_of(p), :]

    begin("ck", "cv0", "cv1")
    with scope("qkv"):
        ready("tok", "gain", "len")
        tok = tok_v[...].astype(F32)
        xn = (normed(tok) * gain_v[...]).astype(BF)
        lens = jnp.broadcast_to(len_v[...].astype(F32), (16, 16))
        diag = iota((16, 16), 0) == iota((16, 16), 1)
        len_c = jnp.sum(jnp.where(diag, lens, 0.0), axis=1, keepdims=True)
        fill_c = len_c - 128.0 * jnp.floor(len_c * (1.0 / 128.0))
        lane = iota((16, 128), 1)
        inverse = jnp.exp((lane % 64).astype(F32) * (-math.log(rope_base) / 64.0))
        sine, cosine = sin_cos(len_c * inverse)
        sine = jnp.where(lane < 64, -sine, sine)
        ready_all("qk", ck)
        raw_q = dot(xn, wq[...])
        raw_k = dot(xn, wk[...])

        def rotate(raw):
            parts = []
            for h in range(4):
                v = raw[:, 128 * h : 128 * h + 128]
                parts.append(v * cosine + pltpu.roll(v, 64, 1) * sine)
            return jnp.concatenate(parts, axis=1)

        queries = (rotate(raw_q) * 128.0 ** (-0.5)).astype(BF)
        new_keys = rotate(raw_k).astype(BF)
        keys_v[...] = new_keys
        results[0].start()
        ready("wv")
        new_values = dot(xn, wv[...]).astype(BF)
        vals_v[...] = new_values
        results[1].start()

    begin("st0", "st1", "st2", "st3", "wo", "fgain")
    with scope("rows"):
        spread_rows = onehot(iota((128, 16), 0) // 8 == iota((128, 16), 1))
        head_512 = iota((128, 512), 0) % 8 == iota((128, 512), 1) // 128
        q_rows = jnp.where(head_512, dot(spread_rows, queries), 0.0)
        own_w = jnp.sum(q_rows * dot(spread_rows, new_keys), axis=-1, keepdims=True)
        own_w = own_w.astype(BF).astype(F32)
        qrows[...] = q_rows
        fill = dot(spread_rows, jnp.broadcast_to(fill_c, (16, 256)).astype(BF))
        row = iota((128, 256), 0)
        col = iota((128, 256), 1)
        head = row % 8
        rate = jnp.full((128, 256), math.log1p(-(2.0 ** -5)), F32)
        for h in range(1, 4):
            rate = jnp.where(head == h, math.log1p(-(2.0 ** (-5 - h))), rate)
        place = (col % 128).astype(F32)
        live = (place < fill) & (col // 128 == (row // 8) % 2)
        decay_v[...] = jnp.where(live, jnp.exp(jnp.maximum(fill - place, 0.0) * rate), 0.0)
        carry = jnp.exp((fill + 1.0) * rate)
        acc_v[...] = own_w * by_head(dot(spread_rows, new_values), 128)

    with scope("barrier"):
        pl.semaphore_wait(barrier, 22)
    with scope("early"):
        for dz, dy in offsets:
            zz, tt = plane(dz, dy)
            mine = wown.at[experts_of(zz * 4 + tt), :]
            remote(mine, wg.at[z, t], w_s.at[0], w_r.at[dz], device(zz, tt)).start()
        pltpu.make_async_copy(dw.at[:, q], dw.at[:, q], loc.at[0]).wait()
        for c in first:
            c.start()
        across.start()

    with scope("scores"):
        ready("ck")
        weights = []
        for i in range(8):
            r = slice(16 * i, 16 * i + 16)
            got = dot_t(qrows[r].astype(BF), ck[2 * i : 2 * i + 2].reshape(256, 512))
            weights.append((got * decay_v[r]).astype(BF))

    begin("sg", "su", "sd", "eg", "eu", "ed", "mix")
    with scope("values"):
        for i in range(8):
            if i % 4 == 0:
                ready(f"cv{i // 4}")
            r = slice(16 * i, 16 * i + 16)
            got = dot(weights[i], cv[2 * i : 2 * i + 2].reshape(256, 1024))
            acc_v[r] = acc_v[r] + by_head(got, 16)

    with scope("state"):
        low = iota((16, 512), 0) < 8
        for i in range(8):
            if i % 2 == 0:
                ready(f"st{i // 2}")
            r = slice(16 * i, 16 * i + 16)
            rows = qrows[r]
            both = jnp.concatenate(
                [jnp.where(low, rows, 0.0), jnp.where(low, 0.0, rows)], axis=1
            ).astype(BF)
            got = dot(both, st[2 * i : 2 * i + 2].reshape(1024, 256).astype(BF))
            acc_v[r] = acc_v[r] + got * carry[r]

    with scope("out"):
        headed = normed(acc_v[...]).astype(BF)
        ready("wo")
        mixed = jnp.zeros((16, 1024), F32)
        for h in range(4):
            pick = onehot(iota((16, 128), 1) == iota((16, 128), 0) * 8 + h)
            mixed = mixed + dot(dot(pick, headed).astype(BF), wo[256 * h : 256 * h + 256])
        residual = tok + normed(mixed)
        ready("fgain")
        xv = (normed(residual) * fgain_v[...]).astype(BF)
        xown[...] = xv
        xg[z, t] = xv
        for dz, dy in offsets:
            dev = device(*plane(dz, dy))
            remote(xown, xg.at[z, t], x_s.at[0], x_r.at[dz], dev).start()

    with scope("shared"):
        ready_all("shared", dw)
        hidden = (silu(dot(xv, sg[...])) * dot(xv, su[...])).astype(BF)
        shared = dot(hidden, sd[...])

    with scope("pump1"):
        arrived(dw.at[:, pl.ds(0, 2)], d_r.at[0])
        for c in second + handed:
            c.start()

    before = onehot(
        (iota((128, 128), 0) < iota((128, 128), 1))
        & (iota((128, 128), 0) // 16 == iota((128, 128), 1) // 16)
    )
    slot = iota((8, 8, 128), 1)
    sender = iota((8, 8, 128), 2) // 16
    picks = {}

    def row_at(dz):
        return lax.rem(z + 4 - dz, 4)

    def dispatch(dz):
        zz = row_at(dz)
        with scope(f"xwait{dz}"):
            count = pl.ds(0, 3 if dz == 0 else 4)
            arrived(wg.at[zz, count], w_r.at[dz])
            arrived(xg.at[zz, count], x_r.at[dz])
        with scope(f"send{dz}"):
            w_p = wg[zz, 0]
            for d in range(1, 4):
                w_p = w_p + pltpu.roll(wg[zz, d], 16 * d, 1)
            r_p = dot(onehot(w_p > 0), before)
            w_b = jnp.broadcast_to(w_p[:, None, :], (8, 8, 128))
            r_b = jnp.broadcast_to(r_p[:, None, :], (8, 8, 128))
            fits = (slot // 2 == sender) & (r_b == (slot % 2).astype(F32))
            picked = jnp.where(fits, w_b, 0.0).reshape(64, 128)
            picks[dz] = picked
            choose = onehot(picked > 0)[:, :64]
            sbuf[zz] = dot(choose, xg[zz].reshape(64, 1024)).astype(BF).reshape(8, 8, 1024)
            for to in reach:
                remote(sbuf.at[zz, to], rbuf.at[zz, q], a_s.at[0], a_r.at[dz], near(to)).start()
            rbuf[zz, q] = sbuf[zz, q]

    def expert(dz):
        zz = row_at(dz)
        with scope(f"ewait{dz}"):
            arrived(rbuf.at[zz, pl.ds(0, 7)], a_r.at[dz])
        with scope(f"expert{dz}"):
            rows = rbuf[zz].reshape(64, 1024)
            hid = (silu(dot(rows, eg[...])) * dot(rows, eu[...])).astype(BF)
            ybuf[zz] = dot(hid, ed[...]).astype(BF).reshape(8, 8, 1024)
            for to in reach:
                remote(ybuf.at[zz, to], bbuf.at[zz, q], b_s.at[0], b_r.at[dz], near(to)).start()
            bbuf[zz, q] = ybuf[zz, q]

    def gather(dz):
        zz = row_at(dz)
        with scope(f"bwait{dz}"):
            arrived(bbuf.at[zz, pl.ds(0, 7)], b_r.at[dz])
        with scope(f"combine{dz}"):
            combine = picks[dz].T[:64]
            comb_hi = combine.astype(BF)
            comb_lo = (combine - comb_hi.astype(F32)).astype(BF)
            back = bbuf[zz].reshape(64, 1024)
            partial = dense_v[zz] + dot(comb_hi, back) + dot(comb_lo, back)
            pbuf[zz] = partial.astype(BF).reshape(4, 16, 1024)
            for dy in (2, 1, 3, 0):
                if (dz, dy) != (0, 0):
                    tt = lax.rem(t + 4 - dy, 4)
                    sums = pbuf.at[zz, tt]
                    remote(sums, qbuf.at[p], p_s.at[0], p_r.at[0], device(zz, tt)).start()

    dispatch(0)
    dispatch(2)
    dispatch(1)
    ready_all("expert", dw)
    expert(0)
    dispatch(3)
    with scope("pump2"):
        arrived(dw.at[:, 0], d_r.at[1])
        third.start()
    expert(2)
    with scope("dwait"):
        arrived(dw.at[:, pl.ds(0, 4)], d_r.at[2])
    with scope("dense"):
        tokens = xg[...].reshape(256, 1024)
        gate = dot_t(tokens, dw[0].reshape(256, 1024))
        raised = dot_t(tokens, dw[1].reshape(256, 1024))
        ready("mix")
        mix = 1.0 / (1.0 + jnp.exp(-mix_v[...]))
        lowered = dot((silu(gate) * raised).astype(BF), dw[2].reshape(256, 1024))
        dense_v[...] = (lowered * mix).reshape(4, 64, 1024)
    expert(1)
    expert(3)
    gather(0)
    gather(2)
    gather(1)
    gather(3)
    qbuf[p] = pbuf[z, t]
    with scope("pwait"):
        arrived(qbuf.at[pl.ds(0, 15)], p_r.at[0])
    with scope("final"):
        total = shared + jnp.sum(qbuf[...].astype(F32), axis=0)
        out_ref[...] = (residual + normed(total)).astype(BF)

    with scope("drain"):
        for c in results:
            c.wait()
        gone(dw.at[:, pl.ds(0, 7)], d_s.at[0])
        gone(wown.at[pl.ds(0, 120), :], w_s.at[0])
        gone(qbuf.at[pl.ds(0, 15)], x_s.at[0])
        gone(sbuf.at[:, pl.ds(0, 7)], a_s.at[0])
        gone(ybuf.at[:, pl.ds(0, 7)], b_s.at[0])
        gone(qbuf.at[pl.ds(0, 15)], p_s.at[0])


def results_kernel(a_in, b_in, c_in, a_out, b_out, c_out, a_v, b_v, c_v, in_s, out_s):
    trio = ((a_in, a_v, a_out), (b_in, b_v, b_out), (c_in, c_v, c_out))
    loads = [pltpu.make_async_copy(i, v, in_s.at[n]) for n, (i, v, _) in enumerate(trio)]
    stores = [pltpu.make_async_copy(v, o, out_s.at[n]) for n, (_, v, o) in enumerate(trio)]
    for c in loads:
        c.start()
    for load, store in zip(loads, stores):
        load.wait()
        store.start()
    for c in stores:
        c.wait()


def per_device(
    tokens, lengths, cache_keys, cache_values, retention_state, mix_gain,
    query_weight, key_weight, value_weight, out_weight, ffn_gain, routes, route_scores,
    expert_gate, expert_up, expert_down, shared_gate, shared_up, shared_down,
    dense_gate, dense_up, dense_down, dense_mix,
):
    vm = pl.BlockSpec(memory_space=pltpu.VMEM)
    hbm = pl.BlockSpec(memory_space=pl.ANY)
    dma = pltpu.SemaphoreType.DMA
    args = (
        tokens, lengths[None, :], mix_gain[None, :], ffn_gain[None, :], dense_mix[None, :],
        routes.T, route_scores.T,
        query_weight, key_weight, value_weight, out_weight,
        cache_keys, cache_values, retention_state.reshape(16, 512, 256),
        expert_gate, expert_up, expert_down, shared_gate, shared_up, shared_down,
        dense_gate, dense_up, dense_down,
    )
    local = [a.shape for a in args[:14]] + [a.shape[-2:] for a in args[14:20]]
    shapes = tuple(jax.ShapeDtypeStruct((16, n), BF) for n in (1024, 512, 1024))
    held = pl.pallas_call(
        layer_kernel,
        out_shape=shapes,
        in_specs=[hbm] * len(args),
        out_specs=(vm, hbm, hbm),
        scratch_shapes=[pltpu.VMEM(s, a.dtype) for s, a in zip(local, args)]
        + [
            pltpu.VMEM((4, 4, 16, 1024), BF),
            pltpu.VMEM((16, 1024), BF),
            pltpu.VMEM((4, 4, 8, 128), F32),
            pltpu.VMEM((128, 128), F32),
            pltpu.VMEM((16, 512), BF),
            pltpu.VMEM((16, 1024), BF),
            pltpu.VMEM((3, 8, 32, 1024), BF),
            pltpu.VMEM((4, 64, 1024), F32),
            pltpu.VMEM((4, 8, 8, 1024), BF),
            pltpu.VMEM((4, 8, 8, 1024), BF),
            pltpu.VMEM((4, 8, 8, 1024), BF),
            pltpu.VMEM((4, 8, 8, 1024), BF),
            pltpu.VMEM((4, 4, 16, 1024), BF),
            pltpu.VMEM((16, 16, 1024), BF),
            pltpu.VMEM((128, 512), F32),
            pltpu.VMEM((128, 256), F32),
            pltpu.VMEM((128, 256), F32),
            dma((3,)), dma((19,)), dma((1,)), dma((4,)), dma((1,)), dma((3,)),
            dma((1,)), dma((4,)), dma((1,)), dma((4,)), dma((1,)), dma((4,)),
            dma((1,)), dma((1,)),
        ],
        compiler_params=pltpu.CompilerParams(collective_id=0, has_side_effects=True),
    )(*args)
    return pl.pallas_call(
        results_kernel,
        out_shape=shapes,
        in_specs=[hbm] * 3,
        out_specs=(hbm,) * 3,
        scratch_shapes=[pltpu.VMEM(a.shape, BF) for a in shapes] + [dma((3,)), dma((3,))],
    )(*held)


def solution(mesh):
    row = P("ep", None)
    cube = P("ep", None, None)
    in_specs = (
        row, P("ep"), cube, cube, P("ep", None, None, None), P(), P(), P(), P(), P(), P(),
        row, row, cube, cube, cube, P(), P(), P(), row, row, row, P(),
    )
    return jax.shard_map(
        per_device, mesh=mesh, in_specs=in_specs, out_specs=(row, row, row), check_vma=False
    )
```
